256 devices in a mesh: sp: 64 (over z, y, core), tp: 4 (over x).
Axes of the slice: x: 4, y: 4, z: 8, core: 2. Of those that a mesh axis runs over, the one named last changes fastest.
Arguments:
- head_input_values: bfloat16 [24576, 4096], P('sp', 'tp'), may hold values from -6 to 6
- group_input_vectors: bfloat16 [24576, 1024], P('sp', 'tp'), may hold values from -6 to 6
- group_readout_vectors: bfloat16 [24576, 1024], P('sp', 'tp'), may hold values from -6 to 6
- output_gate_values: bfloat16 [24576, 4096], P('sp', 'tp'), may hold values from -6 to 6
- step_size_logits: float32 [24576, 64], P('sp', 'tp'), may hold values from -6 to 6
- extra_log_decay: float32 [24576, 64], P('sp', 'tp'), may hold values from -1.2 to 0
- head_input_filter: bfloat16 [4, 4096], P(None, 'tp'), may hold values from -3 to 3
- input_vector_filter: bfloat16 [4, 1024], P(None, 'tp'), may hold values from -3 to 3
- readout_vector_filter: bfloat16 [4, 1024], P(None, 'tp'), may hold values from -3 to 3
- step_size_bias: float32 [64], P('tp'), may hold values from -0.5 to 0.5
- head_rate_logarithm: float32 [64], P('tp'), may hold values from -20 to -1
- direct_path_weight: float32 [64], P('tp'), may hold values from 0 to 3
- group_norm_scale: bfloat16 [4096], P('tp'), may hold values from 0.099609375 to 1.8984375
- mixer_output_weight: bfloat16 [4096, 2048], P('tp'), may hold values from -0.09375 to 0.09375
- residual: bfloat16 [24576, 2048], P(('sp', 'tp')), may hold values from -6 to 6
- first_norm_scale: float32 [2048], replicated, may hold values from 0.1 to 1.9
- first_norm_bias: float32 [2048], replicated, may hold values from -1.5 to 1.5
- routes: int32 [24576, 2], P(('sp', 'tp')), may hold values from 0 to 63, all different within a row; in each aligned block of 96 rows (0 to 95, 96 to 191, ...) at most 5 rows name the same one
- routing_weight: float32 [24576, 2], P(('sp', 'tp')), may hold values from 0.1 to 0.9
- expert_gate_weight: bfloat16 [64, 2048, 1024], P('sp', None, 'tp'), may hold values from -0.125 to 0.125
- expert_up_weight: bfloat16 [64, 2048, 1024], P('sp', None, 'tp'), may hold values from -0.125 to 0.125
- expert_down_weight: bfloat16 [64, 2048, 1024], P('sp', None, 'tp'), may hold values from -0.1875 to 0.1875
- final_norm_scale: float32 [2048], replicated, may hold values from 0.1 to 1.9
- final_norm_bias: float32 [2048], replicated, may hold values from -1.5 to 1.5
Outputs:
- final: bfloat16 [24576, 2048], P(('sp', 'tp'))
The draws below stay inside these ranges and needn't reach their ends.
Inputs may be any that keep to these rules, and one draw needn't show every extreme that they name: `routes`: in the rows of one device no expert is named more than 5 times.
All inputs are finite; a program needn't handle non-finite values.
Results may differ from the reference program's by a relative error of at most 0.012.
Values may be sent and summed in bfloat16 or wider, within the bound.
A program may use at most 128 MiB of HBM per device.

```python
import math
import jax
import jax.numpy as jnp
import numpy as np
from jax import lax

D = 2048
HEAD_COUNT = 64
HEAD_DIM = 64
INNER_WIDTH = 4096
GROUP_COUNT = 8
STATE_WIDTH = 128
TAPS = 4
BLOCK_LENGTH = 128
FFE = 1024
TOPK = 2
EXPERTS = 64
TOK_DEV = 384
TOKEN_COUNT = 24576
CAP = 5
N_SP = 64
N_TP = 4


def draw_step_size_logits(key, part):
    key_noise, key_shift, key_heat = jax.random.split(jax.random.fold_in(key, 11), 3)
    block_list = TOKEN_COUNT // TOK_DEV
    heated = jax.random.bernoulli(key_heat, 0.0625, (block_list, 1, HEAD_COUNT))
    jitter = jax.random.uniform(key_shift, (block_list, 1, HEAD_COUNT), jnp.float32, -0.3, 0.3)
    block_shift = jnp.where(heated, 3.5, -1.0) + jitter
    noise_part = 0.7 * jax.random.normal(key_noise, (block_list, TOK_DEV, HEAD_COUNT), jnp.float32)
    return jnp.clip(noise_part + block_shift, -6.0, 6.0).reshape(TOKEN_COUNT, HEAD_COUNT)


def draw_head_rate_logarithm(key, part):
    key_pick, key_fast, key_slow = jax.random.split(jax.random.fold_in(key, 12), 3)
    chance = 0.5
    quick = jax.random.bernoulli(key_pick, chance, (HEAD_COUNT,))
    fast_rate = jnp.log(jax.random.uniform(key_fast, (HEAD_COUNT,), jnp.float32, 0.05, 0.15))
    slow_rate = jnp.log(jax.random.uniform(key_slow, (HEAD_COUNT,), jnp.float32, 0.9, 1.4)) - jnp.log(jnp.float32(0.6 * TOKEN_COUNT))
    return jnp.where(quick, fast_rate, slow_rate)


def draw_extra_log_decay(key, part):
    random_key_split, key_depth = jax.random.split(jax.random.fold_in(key, 13))
    extra_decay_rows = jax.random.randint(random_key_split, (2, HEAD_COUNT), 0, TOKEN_COUNT)
    cumulative_log_decay = jnp.log(jax.random.uniform(key_depth, (2, HEAD_COUNT), jnp.float32, 0.55, 0.8))
    position_index = jnp.arange(TOKEN_COUNT, dtype=jnp.int32)[:, None]
    summed_output = jnp.zeros((TOKEN_COUNT, HEAD_COUNT), jnp.float32)
    for block_total in range(2):
        summed_output = summed_output + jnp.where(position_index == extra_decay_rows[block_total][None, :], cumulative_log_decay[block_total][None, :], 0.0)
    return summed_output


def level_of(stream_key, extent, cuts, smallest, top_value):
    factor_of = 1.0
    for dim, shards_of in cuts:
        draws = jax.random.uniform(jax.random.fold_in(jax.random.fold_in(stream_key, 6), dim), (shards_of,), jnp.float32, smallest / len(cuts), top_value / len(cuts))
        factor_of = factor_of * jnp.repeat(jnp.exp(draws), extent[dim] // shards_of).reshape((-1,) + (1,) * (len(extent) - 1 - dim))
    return factor_of


def shared_out(key, own, number, rows, count, top, most, lean):
    order = jax.random.permutation(key, count)
    packed, common = load_shares(count, rows * top, most, lean, True), load_shares(count, rows * top, most, lean, False)
    places = jnp.arange(count)

    def named(sizes, turn):
        used = int((sizes > 0).sum())
        fixed = max(1, used // 4)
        passed = fixed + (places - fixed + turn * (used - fixed)) % max(1, count - fixed)
        return jnp.zeros((count,), jnp.int32).at[order[jnp.where(places < fixed, places, passed)]].set(jnp.asarray(sizes, jnp.int32))

    sizes = jnp.where(number % 4 == 0, named(packed, number // 4), named(common, number - number // 4 - 1))
    mixed = jax.random.permutation(jax.random.fold_in(own, 3), count)
    donor, receiver = mixed[0:count // 2 * 2:2], mixed[1:count // 2 * 2:2]
    room = jnp.minimum(sizes[donor] - 1, most - sizes[receiver]) // 2
    room = jnp.where((donor == order[0]) | (receiver == order[0]) | (sizes[receiver] == 0), 0, jnp.maximum(room, 0))
    passed = jax.random.randint(jax.random.fold_in(own, 4), (count // 2,), 0, 1 << 20) % (room + 1)
    sizes = sizes.at[donor].add(-passed).at[receiver].add(passed)
    items = jnp.searchsorted(jnp.cumsum(sizes), jnp.arange(rows * top), side="right").astype(jnp.int32)
    listing = items.reshape(top, rows).T
    listing = listing[jax.random.permutation(jax.random.fold_in(own, 1), rows)]
    turn = jax.random.randint(jax.random.fold_in(own, 2), (rows, 1), 0, top)
    return jnp.take_along_axis(listing, (jnp.arange(top)[None, :] + turn) % top, axis=1)


def load_shares(amount, total, reach, skew, full):
    weights = [(1 << 20) // math.isqrt(standing ** skew) + 1 for standing in range(1, amount + 1)]
    largest = reach if full else min(reach, max(-(-total // amount), total * weights[0] // sum(weights)))
    least = 1 if total - largest >= amount - 1 else 0
    counts, surplus = [largest] + [least] * (amount - 1), total - largest - least * (amount - 1)
    while surplus > 0:
        free = [i for i in range(1, amount) if counts[i] < largest] or [i for i in range(1, amount) if counts[i] < reach]
        pool, left = sum([weights[i] for i in free]), surplus
        for i in free:
            more = min(reach - counts[i], max(1, left * weights[i] // pool), surplus)
            counts[i] = counts[i] + more
            surplus = surplus - more
    return np.array(counts)


def noise(own_key, shape, scale, most, shards=(), kind=jnp.bfloat16):
    result = scale * jax.random.normal(own_key, shape, jnp.float32)
    if shards:
        result = result * level_of(own_key, shape, shards, -0.22, 0.18)
    return jnp.clip(result, -most, most).astype(kind)


def setup_inputs(seed: int = 0) -> dict:
    seeds = jax.random.split(jax.random.key(seed), 25)
    head_input_values = noise(seeds[0], (TOKEN_COUNT, INNER_WIDTH), 1.0, 6.0, ((0, 64), (1, 4)))
    group_input_vectors = noise(seeds[1], (TOKEN_COUNT, GROUP_COUNT * STATE_WIDTH), 1.0, 6.0, ((0, 64), (1, 4)))
    group_readout_vectors = noise(seeds[2], (TOKEN_COUNT, GROUP_COUNT * STATE_WIDTH), 1.0, 6.0, ((0, 64), (1, 4)))
    output_gate_values = noise(seeds[3], (TOKEN_COUNT, INNER_WIDTH), 1.0, 6.0, ((0, 64), (1, 4)))
    step_size_logits = draw_step_size_logits(jax.random.fold_in(seeds[24], 71), 0)
    extra_log_decay = draw_extra_log_decay(jax.random.fold_in(seeds[24], 71), 0)
    head_input_filter = noise(seeds[6], (TAPS, INNER_WIDTH), 0.5, 3.0, ((1, 4),))
    input_vector_filter = noise(seeds[7], (TAPS, GROUP_COUNT * STATE_WIDTH), 0.5, 3.0, ((1, 4),))
    readout_vector_filter = noise(seeds[8], (TAPS, GROUP_COUNT * STATE_WIDTH), 0.5, 3.0, ((1, 4),))
    step_size_bias = jnp.clip(jax.random.uniform(seeds[9], (HEAD_COUNT,), jnp.float32, -0.5, 0.5) * level_of(seeds[9], (HEAD_COUNT,), ((0, 4),), -0.4, 0.0), -0.5, 0.5)
    head_rate_logarithm = draw_head_rate_logarithm(jax.random.fold_in(seeds[24], 71), 0)
    direct_path_weight = jnp.clip(3.0 * jax.random.uniform(seeds[11], (HEAD_COUNT,), jnp.float32) ** level_of(seeds[11], (HEAD_COUNT,), ((0, 4),), -0.2, 0.2), 0.0, 3.0)
    group_norm_scale = jnp.clip(1.0 + 0.18 * jax.random.normal(seeds[12], (INNER_WIDTH,), jnp.float32), 0.099609375, 1.8984375).astype(jnp.bfloat16)
    mixer_output_weight = noise(seeds[13], (INNER_WIDTH, D), INNER_WIDTH ** -0.5, 0.09375, ((0, 4),))
    residual = noise(seeds[14], (TOKEN_COUNT, D), 1.0, 6.0, ((0, 256),))
    first_norm_scale = jnp.clip(1.0 + 0.18 * jax.random.normal(seeds[15], (D,), jnp.float32), 0.1, 1.9)
    first_norm_bias = noise(seeds[16], (D,), 0.3, 1.5, (), jnp.float32)
    routes_keys = jax.random.split(jax.random.fold_in(seeds[17], 1), TOKEN_COUNT // (TOK_DEV // N_TP))
    routes_turns = jax.random.permutation(jax.random.fold_in(seeds[17], 3), TOKEN_COUNT // (TOK_DEV // N_TP))
    routes = jax.vmap(lambda own, number: shared_out(jax.random.fold_in(seeds[17], 2), own, number, TOK_DEV // N_TP, EXPERTS, TOPK, CAP, 2))(routes_keys, routes_turns).reshape((TOKEN_COUNT, TOPK))
    routing_weight = jnp.clip(0.1 + 0.79999997 * jax.random.uniform(seeds[18], (TOKEN_COUNT, TOPK), jnp.float32) ** level_of(seeds[18], (TOKEN_COUNT, TOPK), ((0, 256),), -0.2, 0.2), 0.1, 0.9)
    expert_gate_weight = noise(seeds[19], (EXPERTS, D, FFE), D ** -0.5, 0.125, ((0, 64), (2, 4)))
    expert_up_weight = noise(seeds[20], (EXPERTS, D, FFE), D ** -0.5, 0.125, ((0, 64), (2, 4)))
    expert_down_weight = noise(seeds[21], (EXPERTS, D, FFE), FFE ** -0.5, 0.1875, ((0, 64), (2, 4)))
    final_norm_scale = jnp.clip(1.0 + 0.18 * jax.random.normal(seeds[22], (D,), jnp.float32), 0.1, 1.9)
    final_norm_bias = noise(seeds[23], (D,), 0.3, 1.5, (), jnp.float32)
    return dict(head_input_values=head_input_values, group_input_vectors=group_input_vectors, group_readout_vectors=group_readout_vectors, output_gate_values=output_gate_values, step_size_logits=step_size_logits, extra_log_decay=extra_log_decay, head_input_filter=head_input_filter, input_vector_filter=input_vector_filter, readout_vector_filter=readout_vector_filter, step_size_bias=step_size_bias, head_rate_logarithm=head_rate_logarithm, direct_path_weight=direct_path_weight, group_norm_scale=group_norm_scale, mixer_output_weight=mixer_output_weight, residual=residual, first_norm_scale=first_norm_scale, first_norm_bias=first_norm_bias, routes=routes, routing_weight=routing_weight, expert_gate_weight=expert_gate_weight, expert_up_weight=expert_up_weight, expert_down_weight=expert_down_weight, final_norm_scale=final_norm_scale, final_norm_bias=final_norm_bias)


EPS = 1e-05
ALPHA = 8.0 ** 0.25

def layer_norm(values, gain_row, bias_row):
    mean_value = lax.optimization_barrier(jnp.mean(values, axis=-1, keepdims=True))
    centred = values - mean_value
    spread = lax.optimization_barrier(jnp.mean(centred * centred, axis=-1, keepdims=True))
    return centred * lax.rsqrt(spread + EPS) * gain_row + bias_row

def conv_silu(raw_rows, tail_rows, tap_weights):
    full_rows = jnp.concatenate([tail_rows, raw_rows], axis=0).astype(jnp.float32)
    weights = tap_weights.astype(jnp.float32)
    length = raw_rows.shape[0]
    summed_output = jnp.zeros((length, raw_rows.shape[1]), jnp.float32)
    for offset in range(tap_weights.shape[0]):
        summed_output = summed_output + weights[offset] * full_rows[offset:offset + length]
    return jax.nn.silu(summed_output)

def block_pass(state_now, input_blocks):
    step_scaled_inputs, decay_logarithm, inputs_b, reads_c = input_blocks
    running = jnp.cumsum(decay_logarithm, axis=0)
    running_t = jnp.moveaxis(running, 0, -1)
    length = decay_logarithm.shape[0]
    causal = jnp.arange(length)[:, None] >= jnp.arange(length)[None, :]
    spread_log = jnp.where(causal, running_t[..., :, None] - running_t[..., None, :], -jnp.inf)
    decay_factors = jnp.exp(spread_log)
    decay_products = jnp.einsum('tgn,sgn->gts', reads_c, inputs_b, precision=lax.Precision.HIGHEST)
    within_block_output = jnp.einsum('zmka,azmo->kzmo', decay_products[:, None] * decay_factors, step_scaled_inputs, precision=lax.Precision.HIGHEST)
    carried_in = jnp.einsum('tgn,grpn->tgrp', reads_c, state_now, precision=lax.Precision.HIGHEST) * jnp.exp(running)[..., None]
    to_end = jnp.exp(running_t[..., -1:] - running_t)
    added = jnp.einsum('sgn,grs,sgrp->grpn', inputs_b, to_end, step_scaled_inputs, precision=lax.Precision.HIGHEST)
    state_next = jnp.exp(running_t[..., -1])[..., None, None] * state_now + added
    return (state_next, within_block_output + carried_in)

def slot_layout(block_routes, capacity, experts):
    flat_routes = block_routes.reshape(-1)
    matches = (flat_routes[:, None] == jnp.arange(experts, dtype=jnp.int32)[None, :]).astype(jnp.int32)
    before = jnp.cumsum(matches, axis=0) - matches
    return flat_routes * capacity + lax.optimization_barrier(jnp.sum(before * matches, axis=1))

def partial_layout(capacity, experts):

    def layout_one(block_routes):
        return slot_layout(block_routes, capacity, experts)
    return layout_one

def reference(head_input_values, group_input_vectors, group_readout_vectors, output_gate_values, step_size_logits, extra_log_decay, head_input_filter, input_vector_filter, readout_vector_filter, step_size_bias, head_rate_logarithm, direct_path_weight, group_norm_scale, mixer_output_weight, residual, first_norm_scale, first_norm_bias, routes, routing_weight, expert_gate_weight, expert_up_weight, expert_down_weight, final_norm_scale, final_norm_bias):
    repeat_count = HEAD_COUNT // GROUP_COUNT
    margin = TAPS - 1

    def mixer_block(carry, input_blocks):
        state_now, tail_x, tail_b, tail_c = carry
        unmixed_head_inputs, unmixed_input_vectors, unmixed_readout_vectors, unmixed_gate_values, unmixed_step_sizes, extra_decay_rows = input_blocks
        length = unmixed_head_inputs.shape[0]
        conv_x = conv_silu(unmixed_head_inputs, tail_x, head_input_filter)
        conv_b = conv_silu(unmixed_input_vectors, tail_b, input_vector_filter)
        conv_c = conv_silu(unmixed_readout_vectors, tail_c, readout_vector_filter)
        step_sizes = jax.nn.softplus(unmixed_step_sizes + step_size_bias)
        decay_logarithm = -step_sizes * jnp.exp(head_rate_logarithm) + extra_decay_rows
        heads_x = conv_x.reshape(length, GROUP_COUNT, repeat_count, HEAD_DIM)
        step_scaled_inputs = heads_x * step_sizes.reshape(length, GROUP_COUNT, repeat_count)[..., None]
        state_next, ssm_out = block_pass(state_now, (step_scaled_inputs, decay_logarithm.reshape(length, GROUP_COUNT, repeat_count), conv_b.reshape(length, GROUP_COUNT, STATE_WIDTH), conv_c.reshape(length, GROUP_COUNT, STATE_WIDTH)))
        ssm_out = ssm_out + direct_path_weight.reshape(GROUP_COUNT, repeat_count)[None, :, :, None] * heads_x
        gated = ssm_out.reshape(length, INNER_WIDTH) * jax.nn.silu(unmixed_gate_values.astype(jnp.float32))
        grouped = gated.reshape(length, GROUP_COUNT, -1)
        normed = grouped * lax.rsqrt(lax.optimization_barrier(jnp.mean(grouped * grouped, axis=-1, keepdims=True)) + EPS)
        rows_out = (normed.reshape(length, INNER_WIDTH) * group_norm_scale.astype(jnp.float32)).astype(jnp.bfloat16)
        return ((state_next, unmixed_head_inputs[length - margin:], unmixed_input_vectors[length - margin:], unmixed_readout_vectors[length - margin:]), rows_out)
    block_list = TOKEN_COUNT // BLOCK_LENGTH
    start = (jnp.zeros((GROUP_COUNT, repeat_count, HEAD_DIM, STATE_WIDTH), jnp.float32), jnp.zeros((margin, INNER_WIDTH), jnp.bfloat16), jnp.zeros((margin, GROUP_COUNT * STATE_WIDTH), jnp.bfloat16), jnp.zeros((margin, GROUP_COUNT * STATE_WIDTH), jnp.bfloat16))
    scan_results = (head_input_values.reshape(block_list, BLOCK_LENGTH, INNER_WIDTH), group_input_vectors.reshape(block_list, BLOCK_LENGTH, GROUP_COUNT * STATE_WIDTH), group_readout_vectors.reshape(block_list, BLOCK_LENGTH, GROUP_COUNT * STATE_WIDTH), output_gate_values.reshape(block_list, BLOCK_LENGTH, INNER_WIDTH), step_size_logits.reshape(block_list, BLOCK_LENGTH, HEAD_COUNT), extra_log_decay.reshape(block_list, BLOCK_LENGTH, HEAD_COUNT))
    unused_carry, mixer_rows = lax.scan(mixer_block, start, scan_results)
    mixer_rows = mixer_rows.reshape(TOKEN_COUNT, INNER_WIDTH)
    slice_width = INNER_WIDTH // N_TP
    mixed = jnp.zeros((TOKEN_COUNT, D), jnp.float32)
    for slice_index in range(N_TP):
        partial_value = jnp.dot(mixer_rows[:, slice_index * slice_width:(slice_index + 1) * slice_width], mixer_output_weight[slice_index * slice_width:(slice_index + 1) * slice_width], preferred_element_type=jnp.float32)
        rounded = lax.optimization_barrier(partial_value.astype(jnp.bfloat16))
        mixed = mixed + rounded.astype(jnp.float32)
    middle = layer_norm(ALPHA * residual.astype(jnp.float32) + mixed, first_norm_scale, first_norm_bias).astype(jnp.bfloat16)
    blocks_count = N_SP * N_TP
    rows_block = TOK_DEV // N_TP
    slot_ids = jax.vmap(partial_layout(CAP, EXPERTS))(routes.reshape(blocks_count, rows_block, TOPK))

    def fill_slots(block_rows, block_slots):
        owners = jnp.repeat(jnp.arange(rows_block, dtype=jnp.int32), TOPK)
        source = jnp.full((EXPERTS * CAP,), rows_block, jnp.int32).at[block_slots].set(owners)
        padded = jnp.concatenate([block_rows, jnp.zeros((1, D), jnp.bfloat16)], axis=0)
        return padded[source]
    buffers = jax.vmap(fill_slots)(middle.reshape(blocks_count, rows_block, D), slot_ids)
    buffers = buffers.reshape(blocks_count, EXPERTS, CAP, D)

    def one_expert(expert_index):
        rows_in = lax.dynamic_index_in_dim(buffers, expert_index, 1, keepdims=False).reshape(-1, D)
        weight_gate = lax.dynamic_index_in_dim(expert_gate_weight, expert_index, 0, keepdims=False)
        weight_up = lax.dynamic_index_in_dim(expert_up_weight, expert_index, 0, keepdims=False)
        weight_down = lax.dynamic_index_in_dim(expert_down_weight, expert_index, 0, keepdims=False)
        hidden = (jax.nn.silu(jnp.dot(rows_in, weight_gate, preferred_element_type=jnp.float32)) * jnp.dot(rows_in, weight_up, preferred_element_type=jnp.float32)).astype(jnp.bfloat16)
        return jnp.dot(hidden, weight_down.T, preferred_element_type=jnp.float32).astype(jnp.bfloat16)
    answers = lax.map(one_expert, jnp.arange(EXPERTS, dtype=jnp.int32))
    answers = answers.reshape(EXPERTS, blocks_count, CAP, D).transpose(1, 0, 2, 3).reshape(blocks_count, EXPERTS * CAP, D)

    def take_rows(block_answers, block_slots):
        return block_answers[block_slots]
    picked = jax.vmap(take_rows)(answers, slot_ids).astype(jnp.float32).reshape(TOKEN_COUNT, TOPK, D)
    ffn = lax.optimization_barrier(jnp.sum(picked * routing_weight[..., None], axis=1))
    return layer_norm(ALPHA * middle.astype(jnp.float32) + ffn, final_norm_scale, final_norm_bias).astype(jnp.bfloat16)
```

```python
import functools

import jax
import jax.numpy as jnp
from jax import lax
from jax.experimental import pallas as pl
from jax.experimental.pallas import tpu as pltpu
from jax.sharding import PartitionSpec as P

HEAD_DIM = 64
STATE_WIDTH = 128
BLOCK = 128
EPS = 1e-05
ALPHA = 8.0**0.25
F32 = jnp.float32
BF16 = jnp.bfloat16
VMEM_LIMIT = 62 * 1024 * 1024


def dot(a, b, dims=((1,), (0,)), precision=None):
    return lax.dot_general(
        a, b, (dims, ((), ())), preferred_element_type=F32, precision=precision
    )


def silu(v):
    return v * (1.0 / (1.0 + jnp.exp(-v)))


def layer_norm(values, gain_row, bias_row):
    mean_value = jnp.mean(values, axis=-1, keepdims=True)
    centred = values - mean_value
    spread = jnp.mean(centred * centred, axis=-1, keepdims=True)
    return centred * lax.rsqrt(spread + EPS) * gain_row + bias_row


def remote(src, dst, send, recv, sp=None, tp=None):
    target = {}
    if sp is not None:
        target["sp"] = sp
    if tp is not None:
        target["tp"] = tp
    return pltpu.make_async_remote_copy(
        src_ref=src,
        dst_ref=dst,
        send_sem=send,
        recv_sem=recv,
        device_id=target,
        device_id_type=pl.DeviceIdType.MESH,
    )


def pair_columns(values, pair, low_half):
    rows = values.shape[0]
    first = jnp.broadcast_to(values[:, 2 * pair : 2 * pair + 1], (rows, 128))
    second = jnp.broadcast_to(values[:, 2 * pair + 1 : 2 * pair + 2], (rows, 128))
    return jnp.where(low_half[:rows], first, second)


def mixer_kernel(
    n_sp,
    n_tp,
    x,
    b,
    c,
    gate,
    logits,
    extra,
    fx,
    fb,
    fc,
    bias,
    rate,
    direct,
    gns,
    wout,
    resid,
    n1s,
    n1b,
    mid,
    tail_x,
    tail_b,
    tail_c,
    ext_x,
    ext_b,
    ext_c,
    dec_src,
    dec_recv,
    sl_src,
    sl_recv,
    pf_src,
    pf_recv,
    xs,
    xw,
    cb,
    cc,
    ysg,
    ersg,
    added,
    rows_out,
    partial,
    arrived,
    tail_sems,
    dec_sems,
    sl_sems,
    pf_sems,
    tp_sems,
):
    me = lax.axis_index("sp")
    col = lax.axis_index("tp")
    length, width = x.shape
    n_blocks = length // BLOCK
    pairs = width // 128
    groups = b.shape[1] // STATE_WIDTH
    group_width = width // groups

    after = lax.rem(me + 1, n_sp)
    tails = [
        remote(v.at[pl.ds(length - 8, 8)], t, tail_sems.at[0, i], tail_sems.at[1, i], sp=after)
        for i, (v, t) in enumerate(((x, tail_x), (b, tail_b), (c, tail_c)))
    ]
    for copy in tails:
        copy.start()

    low_half = lax.broadcasted_iota(jnp.int32, (BLOCK, 128), 1) < 64
    row_id = lax.broadcasted_iota(jnp.int32, (BLOCK, BLOCK), 0)
    lane_id = lax.broadcasted_iota(jnp.int32, (BLOCK, BLOCK), 1)
    causal = row_id >= lane_id
    lower = causal.astype(F32)

    raw = logits[...] + bias[...]
    steps = jnp.maximum(raw, 0.0) + jnp.log(1.0 + jnp.exp(-jnp.abs(raw)))
    decay = -steps * jnp.exp(rate[...]) + extra[...]
    running = [
        dot(lower, decay[BLOCK * k : BLOCK * (k + 1)], precision=lax.Precision.HIGHEST)
        for k in range(n_blocks)
    ]
    totals = [r[BLOCK - 1 : BLOCK] for r in running]
    whole = functools.reduce(lambda p, q: p + q, totals)
    for j in range(pairs):
        dec_src[j] = pair_columns(whole, j, low_half)

    def send_decay(d, carry):
        target = lax.rem(me + d, n_sp)
        remote(
            dec_src.at[lax.rem(target, pairs)],
            dec_recv.at[d],
            dec_sems.at[0],
            dec_sems.at[1],
            sp=target,
        ).start()
        return carry

    own_decay = pltpu.make_async_copy(
        dec_src.at[lax.rem(me, pairs)], dec_recv.at[0], dec_sems.at[1]
    )
    own_decay.start()
    lax.fori_loop(1, n_sp, send_decay, 0)

    ext_x[8:, :] = x[...].astype(F32)
    ext_b[8:, :] = b[...].astype(F32)
    ext_c[8:, :] = c[...].astype(F32)
    for copy in tails:
        copy.wait()
    has_tail = (me > 0).astype(F32)
    ext_x[0:8, :] = tail_x[...].astype(F32) * has_tail
    ext_b[0:8, :] = tail_b[...].astype(F32) * has_tail
    ext_c[0:8, :] = tail_c[...].astype(F32) * has_tail

    def conv(ext, taps, k, j):
        lanes = slice(128 * j, 128 * (j + 1))
        total = None
        for i in range(4):
            start = BLOCK * k + 5 + i
            term = taps[i : i + 1, lanes].astype(F32) * ext[start : start + BLOCK, lanes]
            total = term if total is None else total + term
        return silu(total)

    for g in range(groups):
        for k in range(n_blocks):
            rows = slice(BLOCK * k, BLOCK * (k + 1))
            lanes = slice(128 * g, 128 * (g + 1))
            cb[rows, lanes] = conv(ext_b, fb, k, g).astype(BF16)
            cc[rows, lanes] = conv(ext_c, fc, k, g).astype(BF16)

    for k in range(n_blocks):
        rows = slice(BLOCK * k, BLOCK * (k + 1))
        block_steps = steps[rows]
        to_end = block_steps * jnp.exp(totals[k] - running[k])
        for j in range(pairs):
            lanes = slice(128 * j, 128 * (j + 1))
            value = conv(ext_x, fx, k, j)
            xs[rows, lanes] = (value * pair_columns(block_steps, j, low_half)).astype(BF16)
            xw[rows, lanes] = (value * pair_columns(to_end, j, low_half)).astype(BF16)
            ysg[rows, lanes] = value * pair_columns(direct[...], j, low_half)

    keep = [
        jnp.concatenate([pair_columns(jnp.exp(t), j, low_half) for j in range(pairs)], axis=1)
        for t in totals
    ]
    for g in range(groups):
        for k in range(n_blocks):
            rows = slice(BLOCK * k, BLOCK * (k + 1))
            added[k, :, group_width * g : group_width * (g + 1)] = dot(
                cb[rows, 128 * g : 128 * (g + 1)],
                xw[rows, group_width * g : group_width * (g + 1)],
                ((0,), (0,)),
            )
    for i in range(STATE_WIDTH // 16):
        for j in range(pairs):
            lanes = slice(128 * j, 128 * (j + 1))
            state = added[0, 16 * i : 16 * (i + 1), lanes]
            for k in range(1, n_blocks):
                state = keep[k][:, lanes] * state + added[k, 16 * i : 16 * (i + 1), lanes]
            sl_src[pairs * i + j] = state.astype(BF16)

    def send_slice(d, carry):
        target = lax.rem(me + d, n_sp)
        remote(sl_src.at[target], sl_recv.at[d], sl_sems.at[0], sl_sems.at[1], sp=target).start()
        return carry

    own_slice = pltpu.make_async_copy(sl_src.at[me], sl_recv.at[0], sl_sems.at[1])
    own_slice.start()
    lax.fori_loop(1, n_sp, send_slice, 0)

    for k in range(n_blocks):
        rows = slice(BLOCK * k, BLOCK * (k + 1))
        across = running[k].T
        grown = jnp.exp(running[k])
        for g in range(groups):
            lanes_g = slice(128 * g, 128 * (g + 1))
            products = dot(cc[rows, lanes_g], cb[rows, lanes_g], ((1,), (1,)))
            for j in range(g * pairs // groups, (g + 1) * pairs // groups):
                lanes = slice(128 * j, 128 * (j + 1))
                weighed = []
                for h in (2 * j, 2 * j + 1):
                    spread = running[k][:, h : h + 1] - across[h : h + 1, :]
                    factors = jnp.exp(jnp.where(causal, spread, -jnp.inf))
                    weighed.append((products * factors).astype(BF16))
                inputs = xs[rows, lanes]
                zero = jnp.zeros_like(inputs)
                stacked = jnp.concatenate(
                    [jnp.where(low_half, inputs, zero), jnp.where(low_half, zero, inputs)], axis=0
                )
                within = dot(jnp.concatenate(weighed, axis=1), stacked)
                opened = silu(gate[rows, lanes].astype(F32))
                ysg[rows, lanes] = (ysg[rows, lanes] + within) * opened
                ersg[rows, lanes] = pair_columns(grown, j, low_half) * opened

    whole_dec = pltpu.make_async_copy(dec_recv, dec_recv, dec_sems.at[1])
    whole_dec.wait()
    pltpu.make_async_copy(sl_recv, sl_recv, sl_sems.at[1]).wait()

    def scan_step(j, state):
        d = lax.rem(me - j + n_sp, n_sp)
        pf_src[j] = state.astype(BF16)
        return jnp.exp(dec_recv[d]) * state + sl_recv[d].astype(F32)

    lax.fori_loop(0, n_sp, scan_step, jnp.zeros((16, 128), F32))

    def send_prefix(d, carry):
        target = lax.rem(me + d, n_sp)
        remote(pf_src.at[target], pf_recv.at[me], pf_sems.at[0], pf_sems.at[1], sp=target).start()
        return carry

    own_prefix = pltpu.make_async_copy(pf_src.at[me], pf_recv.at[me], pf_sems.at[1])
    own_prefix.start()
    lax.fori_loop(1, n_sp, send_prefix, 0)
    pltpu.make_async_copy(pf_recv, pf_recv, pf_sems.at[1]).wait()

    incoming = jnp.concatenate(
        [
            jnp.concatenate([pf_recv[pairs * i + j] for j in range(pairs)], axis=1)
            for i in range(STATE_WIDTH // 16)
        ],
        axis=0,
    ).astype(F32)
    for k in range(n_blocks):
        rows = slice(BLOCK * k, BLOCK * (k + 1))
        for g in range(groups):
            lanes = slice(group_width * g, group_width * (g + 1))
            carried = dot(cc[rows, 128 * g : 128 * (g + 1)], incoming[:, lanes].astype(BF16))
            gated = ysg[rows, lanes] + carried * ersg[rows, lanes]
            power = jnp.mean(gated * gated, axis=-1, keepdims=True)
            rows_out[rows, lanes] = (
                gated * lax.rsqrt(power + EPS) * gns[:, lanes].astype(F32)
            ).astype(BF16)
        if k + 1 < n_blocks:
            incoming = keep[k] * incoming + added[k]

    part = length // n_tp
    copies = []
    for d in (2, 1, 3, 0):
        target = lax.rem(col + d, n_tp)
        start = pl.multiple_of(target * part, part)
        for q in range(4):
            lanes = slice(512 * q, 512 * (q + 1))
            partial[pl.ds(start, part), lanes] = dot(
                rows_out[pl.ds(start, part), :], wout[:, lanes]
            ).astype(BF16)
        if d:
            copy = remote(
                partial.at[pl.ds(start, part)],
                arrived.at[d - 1],
                tp_sems.at[0, d - 1],
                tp_sems.at[1, d - 1],
                tp=target,
            )
            copy.start()
            copies.append(copy)
    for copy in copies:
        copy.wait()
    own = pl.multiple_of(col * part, part)
    mixed = partial[pl.ds(own, part), :].astype(F32)
    for d in range(n_tp - 1):
        mixed = mixed + arrived[d].astype(F32)
    mid[...] = layer_norm(ALPHA * resid[...].astype(F32) + mixed, n1s[...], n1b[...]).astype(BF16)

    def wait_sent(src, sems):
        remote(src, src, sems.at[0], sems.at[1], sp=after).wait_send()

    wait_sent(dec_recv.at[pl.ds(0, n_sp - 1)], dec_sems)
    wait_sent(sl_src.at[pl.ds(0, n_sp - 1)], sl_sems)
    wait_sent(pf_src.at[pl.ds(0, n_sp - 1)], pf_sems)


def expert_kernel(
    n_sp,
    cap,
    mid,
    routes,
    weights,
    wg,
    wu,
    wd,
    n2s,
    n2b,
    out,
    outgoing,
    received,
    answers,
    returned,
    tokens,
    hidden,
    wg_v,
    wu_v,
    wd_v,
    w_sems,
    there,
    back,
):
    me = lax.axis_index("sp")
    n_rows, width = mid.shape
    slots = n_sp * cap
    chunks = width // 128
    n_tp = wg.shape[0]
    loads = [
        pltpu.make_async_copy(src, dst, w_sems.at[i])
        for i, (src, dst) in enumerate(((wg, wg_v), (wu, wu_v), (wd, wd_v)))
    ]
    for load in loads:
        load.start()

    distance = routes[...] - me
    distance = jnp.where(distance < 0, distance + n_sp, distance)
    expert_id = lax.broadcasted_iota(jnp.int32, (n_rows, n_sp), 1)
    hits = [(expert_id == distance[:, k : k + 1]).astype(F32) for k in range(2)]
    r_id = lax.broadcasted_iota(jnp.int32, (n_rows, n_rows), 0)
    s_id = lax.broadcasted_iota(jnp.int32, (n_rows, n_rows), 1)
    before = dot((s_id < r_id).astype(BF16), (hits[0] + hits[1]).astype(BF16))
    slot_id = lax.broadcasted_iota(jnp.int32, (n_rows, slots), 1)
    at_slot = []
    for k in range(2):
        rank = jnp.sum(before * hits[k], axis=1, keepdims=True).astype(jnp.int32)
        at_slot.append(slot_id == distance[:, k : k + 1] * cap + rank)
    chosen = (at_slot[0] | at_slot[1]).astype(F32).astype(BF16)
    for q in range(4):
        lanes = slice(512 * q, 512 * (q + 1))
        piece = dot(chosen, mid[:, lanes], ((0,), (0,))).astype(BF16)
        outgoing[:, 4 * q : 4 * (q + 1), :] = piece.reshape(slots, 4, 128)

    def send_tokens(d, carry):
        target = lax.rem(me + d, n_sp)
        span = pl.ds(cap * d, cap)
        remote(outgoing.at[span], received.at[span], there.at[0], there.at[1], sp=target).start()
        return carry

    own = pltpu.make_async_copy(outgoing.at[pl.ds(0, cap)], received.at[pl.ds(0, cap)], there.at[1])
    own.start()
    lax.fori_loop(1, n_sp, send_tokens, 0)
    for load in loads:
        load.wait()
    pltpu.make_async_copy(received, received, there.at[1]).wait()

    tokens[...] = received[...].reshape(slots, width)

    def hidden_part(j, carry):
        opened = dot(tokens[...], wg_v[j])
        upward = dot(tokens[...], wu_v[j])
        hidden[j] = (silu(opened) * upward).astype(BF16)
        return carry

    lax.fori_loop(0, n_tp, hidden_part, 0)
    for q in range(width // 256):
        rows = slice(256 * q, 256 * (q + 1))
        total = dot(hidden[0], wd_v[0, rows, :], ((1,), (1,)))
        for j in range(1, n_tp):
            total = total + dot(hidden[j], wd_v[j, rows, :], ((1,), (1,)))
        answers[:, 2 * q : 2 * q + 2, :] = total.astype(BF16).reshape(slots, 2, 128)

    def send_answers(d, carry):
        target = lax.rem(me - d + n_sp, n_sp)
        span = pl.ds(cap * d, cap)
        remote(answers.at[span], returned.at[span], back.at[0], back.at[1], sp=target).start()
        return carry

    own = pltpu.make_async_copy(answers.at[pl.ds(0, cap)], returned.at[pl.ds(0, cap)], back.at[1])
    own.start()
    lax.fori_loop(1, n_sp, send_answers, 0)
    share = jnp.where(at_slot[0], weights[:, 0:1], 0.0) + jnp.where(at_slot[1], weights[:, 1:2], 0.0)
    coarse = share.astype(BF16)
    fine = (share - coarse.astype(F32)).astype(BF16)
    pltpu.make_async_copy(returned, returned, back.at[1]).wait()
    tokens[...] = returned[...].reshape(slots, width)
    ffn = dot(coarse, tokens[...]) + dot(fine, tokens[...])
    out[...] = layer_norm(ALPHA * mid[...].astype(F32) + ffn, n2s[...], n2b[...]).astype(BF16)

    rest = pl.ds(cap, slots - cap)
    for sems in (there, back):
        remote(
            outgoing.at[rest], received.at[rest], sems.at[0], sems.at[1], sp=lax.rem(me + 1, n_sp)
        ).wait_send()


def shards(n_sp, n_tp, *arguments):
    (
        head_input_values,
        group_input_vectors,
        group_readout_vectors,
        output_gate_values,
        step_size_logits,
        extra_log_decay,
        head_input_filter,
        input_vector_filter,
        readout_vector_filter,
        step_size_bias,
        head_rate_logarithm,
        direct_path_weight,
        group_norm_scale,
        mixer_output_weight,
        residual,
        first_norm_scale,
        first_norm_bias,
        routes,
        routing_weight,
        expert_gate_weight,
        expert_up_weight,
        expert_down_weight,
        final_norm_scale,
        final_norm_bias,
    ) = arguments
    gathered = [
        lax.all_gather(w.reshape(w.shape[1:]), "tp")
        for w in (expert_gate_weight, expert_up_weight, expert_down_weight)
    ]
    length, width = head_input_values.shape
    state_lanes = group_input_vectors.shape[1]
    rows_here, features = residual.shape
    n_blocks = length // BLOCK
    pairs = width // 128
    slices = (n_sp, 16, 128)
    vmem = pl.BlockSpec(memory_space=pltpu.VMEM)
    anywhere = pl.BlockSpec(memory_space=pl.ANY)
    dma = pltpu.SemaphoreType.DMA
    middle = pl.pallas_call(
        functools.partial(mixer_kernel, n_sp, n_tp),
        out_shape=jax.ShapeDtypeStruct((rows_here, features), BF16),
        in_specs=[vmem] * 17,
        out_specs=vmem,
        scratch_shapes=[
            pltpu.VMEM((8, width), BF16),
            pltpu.VMEM((8, state_lanes), BF16),
            pltpu.VMEM((8, state_lanes), BF16),
            pltpu.VMEM((length + 8, width), F32),
            pltpu.VMEM((length + 8, state_lanes), F32),
            pltpu.VMEM((length + 8, state_lanes), F32),
            pltpu.VMEM((pairs, 1, 128), F32),
            pltpu.VMEM((n_sp, 1, 128), F32),
            pltpu.VMEM(slices, BF16),
            pltpu.VMEM(slices, BF16),
            pltpu.VMEM(slices, BF16),
            pltpu.VMEM(slices, BF16),
            pltpu.VMEM((length, width), BF16),
            pltpu.VMEM((length, width), BF16),
            pltpu.VMEM((length, state_lanes), BF16),
            pltpu.VMEM((length, state_lanes), BF16),
            pltpu.VMEM((length, width), F32),
            pltpu.VMEM((length, width), F32),
            pltpu.VMEM((n_blocks, STATE_WIDTH, width), F32),
            pltpu.VMEM((length, width), BF16),
            pltpu.VMEM((length, features), BF16),
            pltpu.VMEM((n_tp - 1, rows_here, features), BF16),
            dma((2, 3)),
            dma((2,)),
            dma((2,)),
            dma((2,)),
            dma((2, n_tp - 1)),
        ],
        compiler_params=pltpu.CompilerParams(vmem_limit_bytes=VMEM_LIMIT, has_side_effects=True),
        cost_estimate=pl.CostEstimate(
            flops=40_000_000_000, bytes_accessed=10_000_000, transcendentals=0
        ),
        name="mixer",
    )(
        head_input_values,
        group_input_vectors,
        group_readout_vectors,
        output_gate_values,
        step_size_logits,
        extra_log_decay,
        head_input_filter,
        input_vector_filter,
        readout_vector_filter,
        step_size_bias.reshape(1, -1),
        head_rate_logarithm.reshape(1, -1),
        direct_path_weight.reshape(1, -1),
        group_norm_scale.reshape(1, -1),
        mixer_output_weight,
        residual,
        first_norm_scale.reshape(1, -1),
        first_norm_bias.reshape(1, -1),
    )
    experts = n_sp * expert_gate_weight.shape[0]
    cap = max(2, rows_here * routes.shape[1] * 5 // (3 * experts))
    slots = n_sp * cap
    tiles = (slots, features // 128, 128)
    part = expert_gate_weight.shape[2]
    return pl.pallas_call(
        functools.partial(expert_kernel, n_sp, cap),
        out_shape=jax.ShapeDtypeStruct((rows_here, features), BF16),
        in_specs=[vmem] * 3 + [anywhere] * 3 + [vmem] * 2,
        out_specs=vmem,
        scratch_shapes=[
            pltpu.VMEM(tiles, BF16),
            pltpu.VMEM(tiles, BF16),
            pltpu.VMEM(tiles, BF16),
            pltpu.VMEM(tiles, BF16),
            pltpu.VMEM((slots, features), BF16),
            pltpu.VMEM((n_tp, slots, part), BF16),
            pltpu.VMEM((n_tp, features, part), BF16),
            pltpu.VMEM((n_tp, features, part), BF16),
            pltpu.VMEM((n_tp, features, part), BF16),
            dma((3,)),
            dma((2,)),
            dma((2,)),
        ],
        compiler_params=pltpu.CompilerParams(vmem_limit_bytes=VMEM_LIMIT, has_side_effects=True),
        cost_estimate=pl.CostEstimate(
            flops=40_000_000_000, bytes_accessed=10_000_000, transcendentals=0
        ),
        name="experts",
    )(
        middle,
        routes,
        routing_weight,
        *gathered,
        final_norm_scale.reshape(1, -1),
        final_norm_bias.reshape(1, -1),
    )


def solution(mesh):
    every = P(("sp", "tp"), None)
    placed = (
        *([P("sp", "tp")] * 6),
        *([P(None, "tp")] * 3),
        *([P("tp")] * 4),
        P("tp", None),
        every,
        P(),
        P(),
        every,
        every,
        *([P("sp", None, "tp")] * 3),
        P(),
        P(),
    )
    return jax.shard_map(
        functools.partial(shards, mesh.shape["sp"], mesh.shape["tp"]),
        mesh=mesh,
        in_specs=placed,
        out_specs=every,
        check_vma=False,
    )
```

```python
import functools

import jax
import jax.numpy as jnp
from jax import lax
from jax.experimental import pallas as pl
from jax.experimental.pallas import tpu as pltpu
from jax.sharding import PartitionSpec as P

HEAD_DIM = 64
STATE_WIDTH = 128
BLOCK = 128
EPS = 1e-05
ALPHA = 8.0**0.25
F32 = jnp.float32
BF16 = jnp.bfloat16
VMEM_LIMIT = 62 * 1024 * 1024


def dot(a, b, dims=((1,), (0,)), precision=None):
    return lax.dot_general(
        a, b, (dims, ((), ())), preferred_element_type=F32, precision=precision
    )


def silu(v):
    return v * (1.0 / (1.0 + jnp.exp(-v)))


def layer_norm(values, gain_row, bias_row):
    mean_value = jnp.mean(values, axis=-1, keepdims=True)
    centred = values - mean_value
    spread = jnp.mean(centred * centred, axis=-1, keepdims=True)
    return centred * lax.rsqrt(spread + EPS) * gain_row + bias_row


def remote(src, dst, send, recv, sp=None, tp=None):
    target = {}
    if sp is not None:
        target["sp"] = sp
    if tp is not None:
        target["tp"] = tp
    return pltpu.make_async_remote_copy(
        src_ref=src,
        dst_ref=dst,
        send_sem=send,
        recv_sem=recv,
        device_id=target,
        device_id_type=pl.DeviceIdType.MESH,
    )


def pair_columns(values, pair, low_half):
    rows = values.shape[0]
    first = jnp.broadcast_to(values[:, 2 * pair : 2 * pair + 1], (rows, 128))
    second = jnp.broadcast_to(values[:, 2 * pair + 1 : 2 * pair + 2], (rows, 128))
    return jnp.where(low_half[:rows], first, second)


def fused_kernel(
    n_sp,
    n_tp,
    cap,
    x,
    b,
    c,
    gate,
    logits,
    extra,
    fx,
    fb,
    fc,
    bias,
    rate,
    direct,
    gns,
    resid,
    n1s,
    n1b,
    routes,
    weights,
    n2s,
    n2b,
    wout_h,
    wg,
    wu,
    wd,
    out,
    tail_x,
    tail_b,
    tail_c,
    ext_x,
    ext_b,
    ext_c,
    dec_src,
    dec_recv,
    sl_src,
    sl_recv,
    pf_src,
    pf_recv,
    xs,
    xw,
    cb,
    cc,
    ysg,
    ersg,
    added,
    rows_out,
    partial,
    arrived,
    wout,
    mid,
    outgoing,
    received,
    answers,
    returned,
    tokens,
    hidden,
    wg_v,
    wu_v,
    wd_v,
    tail_sems,
    dec_sems,
    sl_sems,
    pf_sems,
    tp_sems,
    wout_sem,
    w_first,
    w_recv,
    w_relay,
    w_side,
    there,
    back,
):
    me = lax.axis_index("sp")
    col = lax.axis_index("tp")
    core = lax.rem(me, 2)
    beside = col + 1 - 2 * lax.rem(col, 2)
    across_x = n_tp - 1 - col
    sibling = me + 1 - 2 * core
    home = lax.div(col, 2) == core
    moves = tuple(enumerate(((wg, wg_v), (wu, wu_v), (wd, wd_v))))

    def arrival(m, place):
        block = moves[m][1][1].at[place]
        return pltpu.make_async_copy(block, block, w_recv.at[place, m])

    def first_hop(m):
        src, dst = moves[m][1]
        target = jnp.where(home, beside, across_x)
        return remote(src.at[0], dst.at[col], w_first.at[m], w_recv.at[col, m], tp=target)

    def relay(m):
        block = moves[m][1][1].at[across_x]
        return remote(block, block, w_relay.at[m], w_recv.at[across_x, m], tp=beside)

    def sideways(m, place, src=None):
        block = moves[m][1][1].at[place]
        return remote(
            block if src is None else src,
            block,
            w_side.at[place, m],
            w_recv.at[place, m],
            sp=sibling,
        )

    for m in range(3):
        first_hop(m).start()

    @pl.when(home)
    def _():
        for m in range(3):
            src, dst = moves[m][1]
            pltpu.make_async_copy(src.at[0], dst.at[col], w_recv.at[col, m]).start()
            sideways(m, col, src.at[0]).start()

    pltpu.make_async_copy(wout_h, wout, wout_sem).start()
    length, width = x.shape
    n_blocks = length // BLOCK
    pairs = width // 128
    groups = b.shape[1] // STATE_WIDTH
    group_width = width // groups

    after = lax.rem(me + 1, n_sp)
    tails = [
        remote(v.at[pl.ds(length - 8, 8)], t, tail_sems.at[0, i], tail_sems.at[1, i], sp=after)
        for i, (v, t) in enumerate(((x, tail_x), (b, tail_b), (c, tail_c)))
    ]
    for copy in tails:
        copy.start()

    low_half = lax.broadcasted_iota(jnp.int32, (BLOCK, 128), 1) < 64
    row_id = lax.broadcasted_iota(jnp.int32, (BLOCK, BLOCK), 0)
    lane_id = lax.broadcasted_iota(jnp.int32, (BLOCK, BLOCK), 1)
    causal = row_id >= lane_id
    lower = causal.astype(F32)

    raw = logits[...].T + bias[...]
    steps = jnp.maximum(raw, 0.0) + jnp.log(1.0 + jnp.exp(-jnp.abs(raw)))
    decay = -steps * jnp.exp(rate[...]) + extra[...].T
    running = [
        dot(lower, decay[BLOCK * k : BLOCK * (k + 1)], precision=lax.Precision.HIGHEST)
        for k in range(n_blocks)
    ]
    totals = [r[BLOCK - 1 : BLOCK] for r in running]
    whole = functools.reduce(lambda p, q: p + q, totals)
    for j in range(pairs):
        dec_src[j] = pair_columns(whole, j, low_half)

    def send_decay(d, carry):
        target = lax.rem(me + d, n_sp)
        remote(
            dec_src.at[lax.rem(target, pairs)],
            dec_recv.at[d],
            dec_sems.at[0],
            dec_sems.at[1],
            sp=target,
        ).start()
        return carry

    own_decay = pltpu.make_async_copy(
        dec_src.at[lax.rem(me, pairs)], dec_recv.at[0], dec_sems.at[1]
    )
    own_decay.start()
    lax.fori_loop(1, n_sp, send_decay, 0)

    ext_x[8:, :] = x[...].astype(F32)
    ext_b[8:, :] = b[...].astype(F32)
    ext_c[8:, :] = c[...].astype(F32)
    for copy in tails:
        copy.wait()
    has_tail = (me > 0).astype(F32)
    ext_x[0:8, :] = tail_x[...].astype(F32) * has_tail
    ext_b[0:8, :] = tail_b[...].astype(F32) * has_tail
    ext_c[0:8, :] = tail_c[...].astype(F32) * has_tail

    def conv(ext, taps, k, j):
        lanes = slice(128 * j, 128 * (j + 1))
        total = None
        for i in range(4):
            start = BLOCK * k + 5 + i
            term = taps[i : i + 1, lanes].astype(F32) * ext[start : start + BLOCK, lanes]
            total = term if total is None else total + term
        return silu(total)

    for g in range(groups):
        for k in range(n_blocks):
            rows = slice(BLOCK * k, BLOCK * (k + 1))
            lanes = slice(128 * g, 128 * (g + 1))
            cb[rows, lanes] = conv(ext_b, fb, k, g).astype(BF16)
            cc[rows, lanes] = conv(ext_c, fc, k, g).astype(BF16)

    for k in range(n_blocks):
        rows = slice(BLOCK * k, BLOCK * (k + 1))
        block_steps = steps[rows]
        to_end = block_steps * jnp.exp(totals[k] - running[k])
        for j in range(pairs):
            lanes = slice(128 * j, 128 * (j + 1))
            value = conv(ext_x, fx, k, j)
            xs[rows, lanes] = (value * pair_columns(block_steps, j, low_half)).astype(BF16)
            xw[rows, lanes] = (value * pair_columns(to_end, j, low_half)).astype(BF16)
            ysg[rows, lanes] = value * pair_columns(direct[...], j, low_half)

    keep = [
        jnp.concatenate([pair_columns(jnp.exp(t), j, low_half) for j in range(pairs)], axis=1)
        for t in totals
    ]
    for g in range(groups):
        for k in range(n_blocks):
            rows = slice(BLOCK * k, BLOCK * (k + 1))
            added[k, :, group_width * g : group_width * (g + 1)] = dot(
                cb[rows, 128 * g : 128 * (g + 1)],
                xw[rows, group_width * g : group_width * (g + 1)],
                ((0,), (0,)),
            )
    for i in range(STATE_WIDTH // 16):
        for j in range(pairs):
            lanes = slice(128 * j, 128 * (j + 1))
            state = added[0, 16 * i : 16 * (i + 1), lanes]
            for k in range(1, n_blocks):
                state = keep[k][:, lanes] * state + added[k, 16 * i : 16 * (i + 1), lanes]
            sl_src[pairs * i + j] = state.astype(BF16)

    def send_slice(d, carry):
        target = lax.rem(me + d, n_sp)
        remote(sl_src.at[target], sl_recv.at[d], sl_sems.at[0], sl_sems.at[1], sp=target).start()
        return carry

    own_slice = pltpu.make_async_copy(sl_src.at[me], sl_recv.at[0], sl_sems.at[1])
    own_slice.start()
    lax.fori_loop(1, n_sp, send_slice, 0)

    for k in range(n_blocks):
        rows = slice(BLOCK * k, BLOCK * (k + 1))
        across = running[k].T
        grown = jnp.exp(running[k])
        for g in range(groups):
            lanes_g = slice(128 * g, 128 * (g + 1))
            products = dot(cc[rows, lanes_g], cb[rows, lanes_g], ((1,), (1,)))
            for j in range(g * pairs // groups, (g + 1) * pairs // groups):
                lanes = slice(128 * j, 128 * (j + 1))
                weighed = []
                for h in (2 * j, 2 * j + 1):
                    spread = running[k][:, h : h + 1] - across[h : h + 1, :]
                    factors = jnp.exp(jnp.where(causal, spread, -jnp.inf))
                    weighed.append((products * factors).astype(BF16))
                inputs = xs[rows, lanes]
                zero = jnp.zeros_like(inputs)
                stacked = jnp.concatenate(
                    [jnp.where(low_half, inputs, zero), jnp.where(low_half, zero, inputs)], axis=0
                )
                within = dot(jnp.concatenate(weighed, axis=1), stacked)
                opened = silu(gate[rows, lanes].astype(F32))
                ysg[rows, lanes] = (ysg[rows, lanes] + within) * opened
                ersg[rows, lanes] = pair_columns(grown, j, low_half) * opened

    whole_dec = pltpu.make_async_copy(dec_recv, dec_recv, dec_sems.at[1])
    whole_dec.wait()
    pltpu.make_async_copy(sl_recv, sl_recv, sl_sems.at[1]).wait()

    def scan_step(j, state):
        d = lax.rem(me - j + n_sp, n_sp)
        pf_src[j] = state.astype(BF16)
        return jnp.exp(dec_recv[d]) * state + sl_recv[d].astype(F32)

    lax.fori_loop(0, n_sp, scan_step, jnp.zeros((16, 128), F32))

    def send_prefix(d, carry):
        target = lax.rem(me + d, n_sp)
        remote(pf_src.at[target], pf_recv.at[me], pf_sems.at[0], pf_sems.at[1], sp=target).start()
        return carry

    own_prefix = pltpu.make_async_copy(pf_src.at[me], pf_recv.at[me], pf_sems.at[1])
    own_prefix.start()
    lax.fori_loop(1, n_sp, send_prefix, 0)
    pltpu.make_async_copy(pf_recv, pf_recv, pf_sems.at[1]).wait()

    gain = gns[...].astype(F32).reshape(1, width)
    incoming = jnp.concatenate(
        [
            jnp.concatenate([pf_recv[pairs * i + j] for j in range(pairs)], axis=1)
            for i in range(STATE_WIDTH // 16)
        ],
        axis=0,
    ).astype(F32)
    for k in range(n_blocks):
        rows = slice(BLOCK * k, BLOCK * (k + 1))
        for g in range(groups):
            lanes = slice(group_width * g, group_width * (g + 1))
            carried = dot(cc[rows, 128 * g : 128 * (g + 1)], incoming[:, lanes].astype(BF16))
            gated = ysg[rows, lanes] + carried * ersg[rows, lanes]
            power = jnp.mean(gated * gated, axis=-1, keepdims=True)
            rows_out[rows, lanes] = (
                gated * lax.rsqrt(power + EPS) * gain[:, lanes]
            ).astype(BF16)
        if k + 1 < n_blocks:
            incoming = keep[k] * incoming + added[k]

    pltpu.make_async_copy(wout_h, wout, wout_sem).wait()
    part = length // n_tp
    copies = []
    for d in (2, 1, 3, 0):
        target = lax.rem(col + d, n_tp)
        start = pl.multiple_of(target * part, part)
        for q in range(4):
            lanes = slice(512 * q, 512 * (q + 1))
            partial[pl.ds(start, part), lanes] = dot(
                rows_out[pl.ds(start, part), :], wout[:, lanes]
            ).astype(BF16)
        if d:
            copy = remote(
                partial.at[pl.ds(start, part)],
                arrived.at[d - 1],
                tp_sems.at[0, d - 1],
                tp_sems.at[1, d - 1],
                tp=target,
            )
            copy.start()
            copies.append(copy)

    @pl.when(home)
    def _():
        for m in range(3):
            arrival(m, across_x).wait()
            relay(m).start()
            sideways(m, across_x).start()
            arrival(m, beside).wait()
            sideways(m, beside).start()

    for copy in copies:
        copy.wait()
    own = pl.multiple_of(col * part, part)
    mixed = partial[pl.ds(own, part), :].astype(F32)
    for d in range(n_tp - 1):
        mixed = mixed + arrived[d].astype(F32)
    mid[...] = layer_norm(ALPHA * resid[...].astype(F32) + mixed, n1s[...], n1b[...]).astype(BF16)

    n_rows, features = mid.shape
    slots = n_sp * cap
    named = routes[...].astype(F32).T.astype(jnp.int32)
    chip = lax.div(me, 2)
    n_chips = n_sp // 2
    distance = lax.shift_right_logical(named, 1) - chip
    distance = jnp.where(distance < 0, distance + n_chips, distance)
    distance = 2 * distance + jnp.where((named & 1) == lax.div(col, 2), 0, 1)
    shares = weights[...].T
    expert_id = lax.broadcasted_iota(jnp.int32, (n_rows, n_sp), 1)
    hits = [(expert_id == distance[:, k : k + 1]).astype(F32) for k in range(2)]
    r_id = lax.broadcasted_iota(jnp.int32, (n_rows, n_rows), 0)
    s_id = lax.broadcasted_iota(jnp.int32, (n_rows, n_rows), 1)
    before = dot((s_id < r_id).astype(BF16), (hits[0] + hits[1]).astype(BF16))
    slot_id = lax.broadcasted_iota(jnp.int32, (n_rows, slots), 1)
    at_slot = []
    for k in range(2):
        rank = jnp.sum(before * hits[k], axis=1, keepdims=True).astype(jnp.int32)
        at_slot.append(slot_id == distance[:, k : k + 1] * cap + rank)
    chosen = (at_slot[0] | at_slot[1]).astype(F32).astype(BF16)
    for q in range(4):
        lanes = slice(512 * q, 512 * (q + 1))
        piece = dot(chosen, mid[:, lanes], ((0,), (0,))).astype(BF16)
        outgoing[:, 4 * q : 4 * (q + 1), :] = piece.reshape(slots, 4, 128)

    def plane(d):
        return col + lax.rem(d, 2) * (across_x - col)

    def send_tokens(d, carry):
        target = 2 * lax.rem(chip + lax.div(d, 2), n_chips) + core
        span = pl.ds(cap * d, cap)
        remote(
            outgoing.at[span], received.at[span], there.at[0], there.at[1], sp=target, tp=plane(d)
        ).start()
        return carry

    own = pltpu.make_async_copy(outgoing.at[pl.ds(0, cap)], received.at[pl.ds(0, cap)], there.at[1])
    own.start()
    lax.fori_loop(1, n_sp, send_tokens, 0)

    @pl.when(home)
    def _():
        for m in range(3):
            last = n_tp - 1 - beside
            arrival(m, last).wait()
            sideways(m, last).start()
            arrival(m, col).wait()

    @pl.when(jnp.logical_not(home))
    def _():
        for m in range(3):
            for place in range(n_tp):
                arrival(m, place).wait()

    pltpu.make_async_copy(received, received, there.at[1]).wait()

    tokens[...] = received[...].reshape(slots, features)

    def hidden_part(j, carry):
        opened = dot(tokens[...], wg_v[j])
        upward = dot(tokens[...], wu_v[j])
        hidden[j] = (silu(opened) * upward).astype(BF16)
        return carry

    lax.fori_loop(0, n_tp, hidden_part, 0)
    for q in range(features // 256):
        rows = slice(256 * q, 256 * (q + 1))
        total = dot(hidden[0], wd_v[0, rows, :], ((1,), (1,)))
        for j in range(1, n_tp):
            total = total + dot(hidden[j], wd_v[j, rows, :], ((1,), (1,)))
        answers[:, 2 * q : 2 * q + 2, :] = total.astype(BF16).reshape(slots, 2, 128)

    def send_answers(d, carry):
        target = 2 * lax.rem(chip - lax.div(d, 2) + n_chips, n_chips) + core
        span = pl.ds(cap * d, cap)
        remote(
            answers.at[span], returned.at[span], back.at[0], back.at[1], sp=target, tp=plane(d)
        ).start()
        return carry

    own = pltpu.make_async_copy(answers.at[pl.ds(0, cap)], returned.at[pl.ds(0, cap)], back.at[1])
    own.start()
    lax.fori_loop(1, n_sp, send_answers, 0)
    share = jnp.where(at_slot[0], shares[:, 0:1], 0.0) + jnp.where(at_slot[1], shares[:, 1:2], 0.0)
    coarse = share.astype(BF16)
    fine = (share - coarse.astype(F32)).astype(BF16)
    pltpu.make_async_copy(returned, returned, back.at[1]).wait()
    tokens[...] = returned[...].reshape(slots, features)
    ffn = dot(coarse, tokens[...]) + dot(fine, tokens[...])
    out[...] = layer_norm(ALPHA * mid[...].astype(F32) + ffn, n2s[...], n2b[...]).astype(BF16)

    def wait_sent(src, sems):
        remote(src, src, sems.at[0], sems.at[1], sp=after).wait_send()

    wait_sent(dec_recv.at[pl.ds(0, n_sp - 1)], dec_sems)
    wait_sent(sl_src.at[pl.ds(0, n_sp - 1)], sl_sems)
    wait_sent(pf_src.at[pl.ds(0, n_sp - 1)], pf_sems)

    rest = pl.ds(cap, slots - cap)
    for sems in (there, back):
        wait_sent(outgoing.at[rest], sems)
    for m in range(3):
        first_hop(m).wait_send()

    @pl.when(home)
    def _():
        for m in range(3):
            relay(m).wait_send()
            for place in range(n_tp):
                sideways(m, place).wait_send()


def shards(n_sp, n_tp, *arguments):
    (
        head_input_values,
        group_input_vectors,
        group_readout_vectors,
        output_gate_values,
        step_size_logits,
        extra_log_decay,
        head_input_filter,
        input_vector_filter,
        readout_vector_filter,
        step_size_bias,
        head_rate_logarithm,
        direct_path_weight,
        group_norm_scale,
        mixer_output_weight,
        residual,
        first_norm_scale,
        first_norm_bias,
        routes,
        routing_weight,
        expert_gate_weight,
        expert_up_weight,
        expert_down_weight,
        final_norm_scale,
        final_norm_bias,
    ) = arguments
    length, width = head_input_values.shape
    state_lanes = group_input_vectors.shape[1]
    rows_here, features = residual.shape
    n_blocks = length // BLOCK
    pairs = width // 128
    slices = (n_sp, 16, 128)
    vmem = pl.BlockSpec(memory_space=pltpu.VMEM)
    anywhere = pl.BlockSpec(memory_space=pl.ANY)
    dma = pltpu.SemaphoreType.DMA
    experts = n_sp * expert_gate_weight.shape[0]
    cap = max(2, rows_here * routes.shape[1] * 5 // (3 * experts))
    slots = n_sp * cap
    tiles = (slots, features // 128, 128)
    part = expert_gate_weight.shape[2]
    return pl.pallas_call(
        functools.partial(fused_kernel, n_sp, n_tp, cap),
        out_shape=jax.ShapeDtypeStruct((rows_here, features), BF16),
        in_specs=[vmem] * 20 + [anywhere] * 4,
        out_specs=vmem,
        scratch_shapes=[
            pltpu.VMEM((8, width), BF16),
            pltpu.VMEM((8, state_lanes), BF16),
            pltpu.VMEM((8, state_lanes), BF16),
            pltpu.VMEM((length + 8, width), F32),
            pltpu.VMEM((length + 8, state_lanes), F32),
            pltpu.VMEM((length + 8, state_lanes), F32),
            pltpu.VMEM((pairs, 1, 128), F32),
            pltpu.VMEM((n_sp, 1, 128), F32),
            pltpu.VMEM(slices, BF16),
            pltpu.VMEM(slices, BF16),
            pltpu.VMEM(slices, BF16),
            pltpu.VMEM(slices, BF16),
            pltpu.VMEM((length, width), BF16),
            pltpu.VMEM((length, width), BF16),
            pltpu.VMEM((length, state_lanes), BF16),
            pltpu.VMEM((length, state_lanes), BF16),
            pltpu.VMEM((length, width), F32),
            pltpu.VMEM((length, width), F32),
            pltpu.VMEM((n_blocks, STATE_WIDTH, width), F32),
            pltpu.VMEM((length, width), BF16),
            pltpu.VMEM((length, features), BF16),
            pltpu.VMEM((n_tp - 1, rows_here, features), BF16),
            pltpu.VMEM((width, features), BF16),
            pltpu.VMEM((rows_here, features), BF16),
            pltpu.VMEM(tiles, BF16),
            pltpu.VMEM(tiles, BF16),
            pltpu.VMEM(tiles, BF16),
            pltpu.VMEM(tiles, BF16),
            pltpu.VMEM((slots, features), BF16),
            pltpu.VMEM((n_tp, slots, part), BF16),
            pltpu.VMEM((n_tp, features, part), BF16),
            pltpu.VMEM((n_tp, features, part), BF16),
            pltpu.VMEM((n_tp, features, part), BF16),
            dma((2, 3)),
            dma((2,)),
            dma((2,)),
            dma((2,)),
            dma((2, n_tp - 1)),
            dma(()),
            dma((3,)),
            dma((n_tp, 3)),
            dma((3,)),
            dma((n_tp, 3)),
            dma((2,)),
            dma((2,)),
        ],
        compiler_params=pltpu.CompilerParams(vmem_limit_bytes=VMEM_LIMIT, has_side_effects=True),
        name="fused",
    )(
        head_input_values,
        group_input_vectors,
        group_readout_vectors,
        output_gate_values,
        step_size_logits.T,
        extra_log_decay.T,
        head_input_filter,
        input_vector_filter,
        readout_vector_filter,
        step_size_bias.reshape(1, -1),
        head_rate_logarithm.reshape(1, -1),
        direct_path_weight.reshape(1, -1),
        group_norm_scale,
        residual,
        first_norm_scale.reshape(1, -1),
        first_norm_bias.reshape(1, -1),
        routes.T,
        routing_weight.T,
        final_norm_scale.reshape(1, -1),
        final_norm_bias.reshape(1, -1),
        mixer_output_weight,
        expert_gate_weight,
        expert_up_weight,
        expert_down_weight,
    )


def solution(mesh):
    every = P(("sp", "tp"), None)
    placed = (
        *([P("sp", "tp")] * 6),
        *([P(None, "tp")] * 3),
        *([P("tp")] * 4),
        P("tp", None),
        every,
        P(),
        P(),
        every,
        every,
        *([P("sp", None, "tp")] * 3),
        P(),
        P(),
    )
    return jax.shard_map(
        functools.partial(shards, mesh.shape["sp"], mesh.shape["tp"]),
        mesh=mesh,
        in_specs=placed,
        out_specs=every,
        check_vma=False,
    )
```

```python
import functools

import jax
import jax.numpy as jnp
from jax import lax
from jax.experimental import pallas as pl
from jax.experimental.pallas import tpu as pltpu
from jax.sharding import PartitionSpec as P

HEAD_DIM = 64
STATE_WIDTH = 128
BLOCK = 128
EPS = 1e-05
ALPHA = 8.0**0.25
F32 = jnp.float32
BF16 = jnp.bfloat16
VMEM_LIMIT = 62 * 1024 * 1024


def dot(a, b, dims=((1,), (0,)), precision=None):
    return lax.dot_general(
        a, b, (dims, ((), ())), preferred_element_type=F32, precision=precision
    )


def silu(v):
    return v * (1.0 / (1.0 + jnp.exp(-v)))


def layer_norm(values, gain_row, bias_row):
    mean_value = jnp.mean(values, axis=-1, keepdims=True)
    centred = values - mean_value
    spread = jnp.mean(centred * centred, axis=-1, keepdims=True)
    return centred * lax.rsqrt(spread + EPS) * gain_row + bias_row


def remote(src, dst, send, recv, sp=None, tp=None):
    target = {}
    if sp is not None:
        target["sp"] = sp
    if tp is not None:
        target["tp"] = tp
    return pltpu.make_async_remote_copy(
        src_ref=src,
        dst_ref=dst,
        send_sem=send,
        recv_sem=recv,
        device_id=target,
        device_id_type=pl.DeviceIdType.MESH,
    )


def pair_columns(values, pair, low_half):
    rows = values.shape[0]
    first = jnp.broadcast_to(values[:, 2 * pair : 2 * pair + 1], (rows, 128))
    second = jnp.broadcast_to(values[:, 2 * pair + 1 : 2 * pair + 2], (rows, 128))
    return jnp.where(low_half[:rows], first, second)


def fused_kernel(n_sp, n_tp, cap, *refs):
    hbm, out, refs = refs[:24], refs[24], refs[25:]
    loaded, refs = refs[:21], refs[21:]
    (x, b, c, gate, logits, extra, fx, fb, fc, bias, rate, direct, gns, resid) = loaded[:14]
    (n1s, n1b, routes, weights, n2s, n2b, wout) = loaded[14:]
    wg, wu, wd = hbm[21:]
    (
        tail_x,
        tail_b,
        tail_c,
        ext_x,
        ext_b,
        ext_c,
        dec_src,
        dec_recv,
        sl_src,
        sl_recv,
        pf_src,
        pf_recv,
        xs,
        xw,
        cb,
        cc,
        ysg,
        ersg,
        added,
        rows_out,
        partial,
        relayed,
        arrived,
        mid,
        outgoing,
        received,
        answers,
        returned,
        tokens,
        hidden,
        summed,
        wg_v,
        wu_v,
        wd_v,
        load_sems,
        tail_sems,
        dec_sems,
        sl_sems,
        pf_sems,
        tp_sems,
        w_first,
        w_recv,
        w_relay,
        w_side,
        there,
        back,
    ) = refs
    me = lax.axis_index("sp")
    col = lax.axis_index("tp")
    core = lax.rem(me, 2)
    chip = lax.div(me, 2)
    n_chips = n_sp // 2
    beside = col + 1 - 2 * lax.rem(col, 2)
    across_x = n_tp - 1 - col
    last_place = n_tp - 1 - beside
    sibling = me + 1 - 2 * core
    home = lax.div(col, 2) == core
    moves = tuple(enumerate(((wg, wg_v), (wu, wu_v), (wd, wd_v))))
    length, width = x.shape
    n_blocks = length // BLOCK
    pairs = width // 128
    groups = b.shape[1] // STATE_WIDTH
    group_width = width // groups
    n_rows, features = mid.shape
    slots = n_sp * cap

    loads = [
        pltpu.make_async_copy(hbm[i], loaded[i], load_sems.at[i]) for i in range(len(loaded))
    ]
    order = (4, 5, 9, 10, 0, 1, 6, 7, 11, 2, 8, 3, 12, 20, 13, 14, 15, 16, 17, 18, 19)
    for i in order:
        loads[i].start()
    barrier = pltpu.get_barrier_semaphore()

    def greet(sp, tp):
        pl.semaphore_signal(
            barrier, inc=1, device_id={"sp": sp, "tp": tp}, device_id_type=pl.DeviceIdType.MESH
        )

    def greet_column(d, carry):
        greet(lax.rem(me + d, n_sp), col)
        return carry

    def greet_plane(q, carry):
        greet(2 * lax.rem(chip + q, n_chips) + core, across_x)
        return carry

    lax.fori_loop(1, n_sp, greet_column, 0)
    lax.fori_loop(0, n_chips, greet_plane, 0)
    greet(me, beside)
    greet(me, last_place)

    def arrival(m, place):
        block = moves[m][1][1].at[place]
        return pltpu.make_async_copy(block, block, w_recv.at[place, m])

    def first_hop(m):
        src, dst = moves[m][1]
        target = jnp.where(home, beside, across_x)
        return remote(src.at[0], dst.at[col], w_first.at[m], w_recv.at[col, m], tp=target)

    def relay(m):
        block = moves[m][1][1].at[across_x]
        return remote(block, block, w_relay.at[m], w_recv.at[across_x, m], tp=beside)

    def sideways(m, place, src=None):
        block = moves[m][1][1].at[place]
        return remote(
            block if src is None else src,
            block,
            w_side.at[place, m],
            w_recv.at[place, m],
            sp=sibling,
        )

    low_half = lax.broadcasted_iota(jnp.int32, (BLOCK, 128), 1) < 64
    row_id = lax.broadcasted_iota(jnp.int32, (BLOCK, BLOCK), 0)
    lane_id = lax.broadcasted_iota(jnp.int32, (BLOCK, BLOCK), 1)
    causal = row_id >= lane_id
    lower = causal.astype(F32)

    for i in (4, 5, 9, 10):
        loads[i].wait()
    raw = logits[...].T + bias[...]
    steps = jnp.maximum(raw, 0.0) + jnp.log(1.0 + jnp.exp(-jnp.abs(raw)))
    decay = -steps * jnp.exp(rate[...]) + extra[...].T
    running = [
        dot(lower, decay[BLOCK * k : BLOCK * (k + 1)], precision=lax.Precision.HIGHEST)
        for k in range(n_blocks)
    ]
    totals = [r[BLOCK - 1 : BLOCK] for r in running]
    whole = functools.reduce(lambda p, q: p + q, totals)
    for j in range(pairs):
        dec_src[j] = pair_columns(whole, j, low_half)

    for i in (0, 1, 6, 7):
        loads[i].wait()
    ext_x[8:, :] = x[...].astype(F32)
    ext_b[8:, :] = b[...].astype(F32)

    def conv(ext, taps, k, j):
        lanes = slice(128 * j, 128 * (j + 1))
        total = None
        for i in range(4):
            start = BLOCK * k + 5 + i
            term = taps[i : i + 1, lanes].astype(F32) * ext[start : start + BLOCK, lanes]
            total = term if total is None else total + term
        return silu(total)

    def inputs_of_block(k):
        rows = slice(BLOCK * k, BLOCK * (k + 1))
        for g in range(groups):
            cb[rows, 128 * g : 128 * (g + 1)] = conv(ext_b, fb, k, g).astype(BF16)
        to_end = steps[rows] * jnp.exp(totals[k] - running[k])
        for j in range(pairs):
            lanes = slice(128 * j, 128 * (j + 1))
            value = conv(ext_x, fx, k, j)
            ysg[rows, lanes] = value
            xw[rows, lanes] = (value * pair_columns(to_end, j, low_half)).astype(BF16)
        for g in range(groups):
            lanes = slice(group_width * g, group_width * (g + 1))
            added[k, :, lanes] = dot(
                cb[rows, 128 * g : 128 * (g + 1)], xw[rows, lanes], ((0,), (0,))
            )

    for k in range(n_blocks - 1, 0, -1):
        inputs_of_block(k)

    loads[2].wait()
    pl.semaphore_wait(barrier, n_sp - 1 + n_chips + 2)
    after = lax.rem(me + 1, n_sp)
    tails = [
        remote(v.at[pl.ds(length - 8, 8)], t, tail_sems.at[0, i], tail_sems.at[1, i], sp=after)
        for i, (v, t) in enumerate(((x, tail_x), (b, tail_b), (c, tail_c)))
    ]
    for copy in tails:
        copy.start()
    for m in range(3):
        first_hop(m).start()

    @pl.when(home)
    def _():
        for m in range(3):
            src, dst = moves[m][1]
            pltpu.make_async_copy(src.at[0], dst.at[col], w_recv.at[col, m]).start()
            sideways(m, col, src.at[0]).start()

    def send_decay(d, carry):
        target = lax.rem(me + d, n_sp)
        remote(
            dec_src.at[lax.rem(target, pairs)],
            dec_recv.at[d],
            dec_sems.at[0],
            dec_sems.at[1],
            sp=target,
        ).start()
        return carry

    own_decay = pltpu.make_async_copy(
        dec_src.at[lax.rem(me, pairs)], dec_recv.at[0], dec_sems.at[1]
    )
    own_decay.start()
    lax.fori_loop(1, n_sp, send_decay, 0)

    keep = [
        jnp.concatenate([pair_columns(jnp.exp(t), j, low_half) for j in range(pairs)], axis=1)
        for t in totals
    ]

    for copy in tails:
        copy.wait()
    has_tail = (me > 0).astype(F32)
    ext_x[0:8, :] = tail_x[...].astype(F32) * has_tail
    ext_b[0:8, :] = tail_b[...].astype(F32) * has_tail
    inputs_of_block(0)

    for i in range(STATE_WIDTH // 16):
        for j in range(pairs):
            lanes = slice(128 * j, 128 * (j + 1))
            state = added[0, 16 * i : 16 * (i + 1), lanes]
            for k in range(1, n_blocks):
                state = keep[k][:, lanes] * state + added[k, 16 * i : 16 * (i + 1), lanes]
            sl_src[pairs * i + j] = state.astype(BF16)

    def send_slice(d, carry):
        target = lax.rem(me + d, n_sp)
        remote(sl_src.at[target], sl_recv.at[d], sl_sems.at[0], sl_sems.at[1], sp=target).start()
        return carry

    own_slice = pltpu.make_async_copy(sl_src.at[me], sl_recv.at[0], sl_sems.at[1])
    own_slice.start()
    lax.fori_loop(1, n_sp, send_slice, 0)

    for i in (8, 11, 3):
        loads[i].wait()
    ext_c[8:, :] = c[...].astype(F32)
    ext_c[0:8, :] = tail_c[...].astype(F32) * has_tail
    for k in range(n_blocks):
        rows = slice(BLOCK * k, BLOCK * (k + 1))
        across = running[k].T
        grown = jnp.exp(running[k])
        for g in range(groups):
            lanes_g = slice(128 * g, 128 * (g + 1))
            cc[rows, lanes_g] = conv(ext_c, fc, k, g).astype(BF16)
            products = dot(cc[rows, lanes_g], cb[rows, lanes_g], ((1,), (1,)))
            for j in range(g * pairs // groups, (g + 1) * pairs // groups):
                lanes = slice(128 * j, 128 * (j + 1))
                weighed = []
                for h in (2 * j, 2 * j + 1):
                    spread = running[k][:, h : h + 1] - across[h : h + 1, :]
                    factors = jnp.exp(jnp.where(causal, spread, -jnp.inf))
                    weighed.append((products * factors).astype(BF16))
                value = ysg[rows, lanes]
                inputs = (value * pair_columns(steps[rows], j, low_half)).astype(BF16)
                zero = jnp.zeros_like(inputs)
                stacked = jnp.concatenate(
                    [jnp.where(low_half, inputs, zero), jnp.where(low_half, zero, inputs)], axis=0
                )
                within = dot(jnp.concatenate(weighed, axis=1), stacked)
                opened = silu(gate[rows, lanes].astype(F32))
                passed = value * pair_columns(direct[...], j, low_half)
                ysg[rows, lanes] = (passed + within) * opened
                ersg[rows, lanes] = pair_columns(grown, j, low_half) * opened

    pltpu.make_async_copy(dec_recv, dec_recv, dec_sems.at[1]).wait()
    pltpu.make_async_copy(sl_recv, sl_recv, sl_sems.at[1]).wait()

    def scan_step(j, state):
        d = lax.rem(me - j + n_sp, n_sp)
        pf_src[j] = state.astype(BF16)
        return jnp.exp(dec_recv[d]) * state + sl_recv[d].astype(F32)

    lax.fori_loop(0, n_sp, scan_step, jnp.zeros((16, 128), F32))

    def send_prefix(d, carry):
        target = lax.rem(me + d, n_sp)
        remote(pf_src.at[target], pf_recv.at[me], pf_sems.at[0], pf_sems.at[1], sp=target).start()
        return carry

    own_prefix = pltpu.make_async_copy(pf_src.at[me], pf_recv.at[me], pf_sems.at[1])
    own_prefix.start()
    lax.fori_loop(1, n_sp, send_prefix, 0)
    for i in (12, 20, 13, 14, 15, 16, 17, 18, 19):
        loads[i].wait()

    named = routes[...].astype(F32).T.astype(jnp.int32)
    distance = lax.shift_right_logical(named, 1) - chip
    distance = jnp.where(distance < 0, distance + n_chips, distance)
    near = lax.shift_right_logical(distance, 2)
    block = 4 * near + 2 * (distance & 1) + jnp.where((named & 1) == lax.div(col, 2), 0, 1)
    block = block + (n_sp // 2) * lax.shift_right_logical(distance & 3, 1)
    shares = weights[...].T
    expert_id = lax.broadcasted_iota(jnp.int32, (n_rows, n_sp), 1)
    hits = [(expert_id == block[:, k : k + 1]).astype(F32) for k in range(2)]
    r_id = lax.broadcasted_iota(jnp.int32, (n_rows, n_rows), 0)
    s_id = lax.broadcasted_iota(jnp.int32, (n_rows, n_rows), 1)
    before = dot((s_id < r_id).astype(BF16), (hits[0] + hits[1]).astype(BF16))
    slot_id = lax.broadcasted_iota(jnp.int32, (n_rows, slots), 1)
    at_slot = []
    for k in range(2):
        rank = jnp.sum(before * hits[k], axis=1, keepdims=True).astype(jnp.int32)
        at_slot.append(slot_id == block[:, k : k + 1] * cap + rank)
    chosen = (at_slot[0] | at_slot[1]).astype(F32).astype(BF16)
    share = jnp.where(at_slot[0], shares[:, 0:1], 0.0) + jnp.where(at_slot[1], shares[:, 1:2], 0.0)
    coarse = share.astype(BF16)
    fine = (share - coarse.astype(F32)).astype(BF16)
    gain = gns[...].astype(F32).reshape(1, width)

    pltpu.make_async_copy(pf_recv, pf_recv, pf_sems.at[1]).wait()

    incoming = jnp.concatenate(
        [
            jnp.concatenate([pf_recv[pairs * i + j] for j in range(pairs)], axis=1)
            for i in range(STATE_WIDTH // 16)
        ],
        axis=0,
    ).astype(F32)
    for k in range(n_blocks):
        rows = slice(BLOCK * k, BLOCK * (k + 1))
        for g in range(groups):
            lanes = slice(group_width * g, group_width * (g + 1))
            carried = dot(cc[rows, 128 * g : 128 * (g + 1)], incoming[:, lanes].astype(BF16))
            gated = ysg[rows, lanes] + carried * ersg[rows, lanes]
            power = jnp.mean(gated * gated, axis=-1, keepdims=True)
            rows_out[rows, lanes] = (gated * lax.rsqrt(power + EPS) * gain[:, lanes]).astype(BF16)
        if k + 1 < n_blocks:
            incoming = keep[k] * incoming + added[k]

    part = length // n_tp
    half = part // 2
    right, left = lax.rem(col + 1, n_tp), lax.rem(col + n_tp - 1, n_tp)
    opposite = lax.rem(col + 2, n_tp)

    def project(target):
        start = pl.multiple_of(target * part, part)
        for q in range(4):
            lanes = slice(512 * q, 512 * (q + 1))
            partial[pl.ds(start, part), lanes] = dot(
                rows_out[pl.ds(start, part), :], wout[:, lanes]
            ).astype(BF16)

    def half_of(target, which):
        return pl.ds(pl.multiple_of(target * part + which * half, half), half)

    def pass_on(i, rows, dst, target):
        return remote(
            partial.at[rows], dst, tp_sems.at[0, i], tp_sems.at[1, i], tp=target
        )

    project(opposite)
    outward = [
        pass_on(0, half_of(opposite, 0), relayed.at[0], right),
        pass_on(1, half_of(opposite, 1), relayed.at[1], left),
    ]
    for copy in outward:
        copy.start()
    project(right)
    direct_right = pass_on(2, half_of(right, 1), arrived.at[0], right)
    direct_right.start()
    project(left)
    direct_left = pass_on(3, half_of(left, 0), arrived.at[1], left)
    direct_left.start()
    outward[0].wait()
    rows = half_of(right, 0)
    partial[rows, :] = (partial[rows, :].astype(F32) + relayed[0].astype(F32)).astype(BF16)
    joined_right = pass_on(4, rows, arrived.at[2], right)
    joined_right.start()
    outward[1].wait()
    rows = half_of(left, 1)
    partial[rows, :] = (partial[rows, :].astype(F32) + relayed[1].astype(F32)).astype(BF16)
    joined_left = pass_on(5, rows, arrived.at[3], left)
    joined_left.start()
    project(col)

    @pl.when(home)
    def _():
        for m in range(3):
            arrival(m, across_x).wait()
            relay(m).start()
            sideways(m, across_x).start()
            arrival(m, beside).wait()
            sideways(m, beside).start()

    for copy in (direct_right, direct_left, joined_right, joined_left):
        copy.wait()
    for which in range(2):
        rows = half_of(col, which)
        span = slice(half * which, half * (which + 1))
        mixed = partial[rows, :].astype(F32)
        mixed = mixed + arrived[1 - which].astype(F32) + arrived[2 + which].astype(F32)
        mid[span, :] = layer_norm(
            ALPHA * resid[span, :].astype(F32) + mixed, n1s[...], n1b[...]
        ).astype(BF16)

    for q in range(4):
        lanes = slice(512 * q, 512 * (q + 1))
        piece = dot(chosen, mid[:, lanes], ((0,), (0,))).astype(BF16)
        outgoing[:, 4 * q : 4 * (q + 1), :] = piece.reshape(slots, 4, 128)

    def place_of(d):
        r = lax.rem(d, n_sp // 2)
        quarter = 4 * lax.div(r, 4) + 2 * lax.div(d, n_sp // 2) + lax.rem(lax.div(r, 2), 2)
        return quarter, col + lax.rem(d, 2) * (across_x - col)

    n_parts = 2
    blocks = n_sp // n_parts
    piece_rows = blocks * cap

    def send_tokens(d, carry):
        quarter, plane = place_of(d)
        span = pl.ds(cap * d, cap)
        remote(
            outgoing.at[span],
            received.at[span],
            there.at[0],
            there.at[1 + lax.div(d, blocks)],
            sp=2 * lax.rem(chip + quarter, n_chips) + core,
            tp=plane,
        ).start()
        return carry

    def send_answers(d, carry):
        quarter, plane = place_of(d)
        span = pl.ds(cap * d, cap)
        remote(
            answers.at[span],
            returned.at[span],
            back.at[0],
            back.at[1],
            sp=2 * lax.rem(chip - quarter + n_chips, n_chips) + core,
            tp=plane,
        ).start()
        return carry

    own = pltpu.make_async_copy(outgoing.at[pl.ds(0, cap)], received.at[pl.ds(0, cap)], there.at[1])
    own.start()
    lax.fori_loop(1, n_sp, send_tokens, 0)

    def hidden_part(place):
        opened = dot(tokens[...], wg_v[place])
        upward = dot(tokens[...], wu_v[place])
        hidden[place] = (silu(opened) * upward).astype(BF16)

    early = (col, beside, across_x)

    def early_place(i):
        return jnp.where(i == 0, early[0], jnp.where(i == 1, early[1], early[2]))

    def early_hidden(i, carry):
        hidden_part(early_place(i))
        return carry

    def down(place, rows):
        return dot(hidden[place], wd_v[place, rows, :], ((1,), (1,)))

    def early_down():
        def chunk(q, carry):
            rows = pl.ds(pl.multiple_of(256 * q, 256), 256)
            total = down(early[0], rows) + down(early[1], rows) + down(early[2], rows)
            summed[q] = total
            return carry

        lax.fori_loop(0, features // 256, chunk, 0)

    def late_down(first_row):
        for q in range(features // 256):
            total = summed[q] + down(last_place, slice(256 * q, 256 * (q + 1)))
            answers[first_row : first_row + piece_rows, 2 * q : 2 * q + 2, :] = total.astype(
                BF16
            ).reshape(piece_rows, 2, 128)

    @pl.when(home)
    def _():
        for m in range(3):
            arrival(m, col).wait()

    @pl.when(jnp.logical_not(home))
    def _():
        for m in range(3):
            for place in early:
                arrival(m, place).wait()

    for p in range(n_parts):
        span = pl.ds(piece_rows * p, piece_rows)
        pltpu.make_async_copy(received.at[span], received.at[span], there.at[1 + p]).wait()
        tokens[...] = received[span].reshape(piece_rows, features)
        lax.fori_loop(0, 3, early_hidden, 0)
        early_down()
        if p == 0:
            for m in range(3):
                arrival(m, last_place).wait()

                @pl.when(home)
                def _():
                    sideways(m, last_place).start()

        hidden_part(last_place)
        late_down(piece_rows * p)
        if p == 0:
            own = pltpu.make_async_copy(
                answers.at[pl.ds(0, cap)], returned.at[pl.ds(0, cap)], back.at[1]
            )
            own.start()
        lax.fori_loop(max(1, blocks * p), blocks * (p + 1), send_answers, 0)

    pltpu.make_async_copy(returned, returned, back.at[1]).wait()
    back_rows = returned[...].reshape(slots, features)
    ffn = dot(coarse, back_rows) + dot(fine, back_rows)
    out[...] = layer_norm(ALPHA * mid[...].astype(F32) + ffn, n2s[...], n2b[...]).astype(BF16)

    def wait_sent(src, sem):
        remote(src, src, sem, sem, sp=after).wait_send()

    wait_sent(dec_recv.at[pl.ds(0, n_sp - 1)], dec_sems.at[0])
    wait_sent(sl_src.at[pl.ds(0, n_sp - 1)], sl_sems.at[0])
    wait_sent(pf_src.at[pl.ds(0, n_sp - 1)], pf_sems.at[0])
    rest = pl.ds(cap, slots - cap)
    wait_sent(outgoing.at[rest], there.at[0])
    wait_sent(answers.at[rest], back.at[0])
    for m in range(3):
        first_hop(m).wait_send()

    @pl.when(home)
    def _():
        for m in range(3):
            relay(m).wait_send()
            for place in range(n_tp):
                sideways(m, place).wait_send()


def shards(n_sp, n_tp, *arguments):
    (
        head_input_values,
        group_input_vectors,
        group_readout_vectors,
        output_gate_values,
        step_size_logits,
        extra_log_decay,
        head_input_filter,
        input_vector_filter,
        readout_vector_filter,
        step_size_bias,
        head_rate_logarithm,
        direct_path_weight,
        group_norm_scale,
        mixer_output_weight,
        residual,
        first_norm_scale,
        first_norm_bias,
        routes,
        routing_weight,
        expert_gate_weight,
        expert_up_weight,
        expert_down_weight,
        final_norm_scale,
        final_norm_bias,
    ) = arguments
    length, width = head_input_values.shape
    state_lanes = group_input_vectors.shape[1]
    rows_here, features = residual.shape
    n_blocks = length // BLOCK
    pairs = width // 128
    slices = (n_sp, 16, 128)
    vmem = pl.BlockSpec(memory_space=pltpu.VMEM)
    anywhere = pl.BlockSpec(memory_space=pl.ANY)
    dma = pltpu.SemaphoreType.DMA
    experts = n_sp * expert_gate_weight.shape[0]
    cap = max(2, rows_here * routes.shape[1] * 5 // (3 * experts))
    slots = n_sp * cap
    tiles = (slots, features // 128, 128)
    part = expert_gate_weight.shape[2]
    operands = (
        head_input_values,
        group_input_vectors,
        group_readout_vectors,
        output_gate_values,
        step_size_logits.T,
        extra_log_decay.T,
        head_input_filter,
        input_vector_filter,
        readout_vector_filter,
        step_size_bias.reshape(1, -1),
        head_rate_logarithm.reshape(1, -1),
        direct_path_weight.reshape(1, -1),
        group_norm_scale,
        residual,
        first_norm_scale.reshape(1, -1),
        first_norm_bias.reshape(1, -1),
        routes.T,
        routing_weight.T,
        final_norm_scale.reshape(1, -1),
        final_norm_bias.reshape(1, -1),
        mixer_output_weight,
        expert_gate_weight,
        expert_up_weight,
        expert_down_weight,
    )
    return pl.pallas_call(
        functools.partial(fused_kernel, n_sp, n_tp, cap),
        out_shape=jax.ShapeDtypeStruct((rows_here, features), BF16),
        in_specs=[anywhere] * len(operands),
        out_specs=vmem,
        scratch_shapes=[
            *(pltpu.VMEM(v.shape, v.dtype) for v in operands[:21]),
            pltpu.VMEM((8, width), BF16),
            pltpu.VMEM((8, state_lanes), BF16),
            pltpu.VMEM((8, state_lanes), BF16),
            pltpu.VMEM((length + 8, width), F32),
            pltpu.VMEM((length + 8, state_lanes), F32),
            pltpu.VMEM((length + 8, state_lanes), F32),
            pltpu.VMEM((pairs, 1, 128), F32),
            pltpu.VMEM((n_sp, 1, 128), F32),
            pltpu.VMEM(slices, BF16),
            pltpu.VMEM(slices, BF16),
            pltpu.VMEM(slices, BF16),
            pltpu.VMEM(slices, BF16),
            pltpu.VMEM((length, width), BF16),
            pltpu.VMEM((length, width), BF16),
            pltpu.VMEM((length, state_lanes), BF16),
            pltpu.VMEM((length, state_lanes), BF16),
            pltpu.VMEM((length, width), F32),
            pltpu.VMEM((length, width), F32),
            pltpu.VMEM((n_blocks, STATE_WIDTH, width), F32),
            pltpu.VMEM((length, width), BF16),
            pltpu.VMEM((length, features), BF16),
            pltpu.VMEM((2, rows_here // 2, features), BF16),
            pltpu.VMEM((4, rows_here // 2, features), BF16),
            pltpu.VMEM((rows_here, features), BF16),
            pltpu.VMEM(tiles, BF16),
            pltpu.VMEM(tiles, BF16),
            pltpu.VMEM(tiles, BF16),
            pltpu.VMEM(tiles, BF16),
            pltpu.VMEM((slots // 2, features), BF16),
            pltpu.VMEM((n_tp, slots // 2, part), BF16),
            pltpu.VMEM((features // 256, slots // 2, 256), F32),
            pltpu.VMEM((n_tp, features, part), BF16),
            pltpu.VMEM((n_tp, features, part), BF16),
            pltpu.VMEM((n_tp, features, part), BF16),
            dma((21,)),
            dma((2, 3)),
            dma((2,)),
            dma((2,)),
            dma((2,)),
            dma((2, 6)),
            dma((3,)),
            dma((n_tp, 3)),
            dma((3,)),
            dma((n_tp, 3)),
            dma((3,)),
            dma((2,)),
        ],
        compiler_params=pltpu.CompilerParams(
            vmem_limit_bytes=VMEM_LIMIT, has_side_effects=True, collective_id=0
        ),
        name="fused",
    )(*operands)


def solution(mesh):
    every = P(("sp", "tp"), None)
    placed = (
        *([P("sp", "tp")] * 6),
        *([P(None, "tp")] * 3),
        *([P("tp")] * 4),
        P("tp", None),
        every,
        P(),
        P(),
        every,
        every,
        *([P("sp", None, "tp")] * 3),
        P(),
        P(),
    )
    return jax.shard_map(
        functools.partial(shards, mesh.shape["sp"], mesh.shape["tp"]),
        mesh=mesh,
        in_specs=placed,
        out_specs=every,
        check_vma=False,
    )
```

```python
import functools

import jax
import jax.numpy as jnp
from jax import lax
from jax.experimental import pallas as pl
from jax.experimental.pallas import tpu as pltpu
from jax.sharding import PartitionSpec as P

HEAD_DIM = 64
STATE_WIDTH = 128
BLOCK = 128
EPS = 1e-05
ALPHA = 8.0**0.25
F32 = jnp.float32
BF16 = jnp.bfloat16
VMEM_LIMIT = 62 * 1024 * 1024


def dot(a, b, dims=((1,), (0,)), precision=None):
    return lax.dot_general(
        a, b, (dims, ((), ())), preferred_element_type=F32, precision=precision
    )


def silu(v):
    return v * (1.0 / (1.0 + jnp.exp(-v)))


def layer_norm(values, gain_row, bias_row):
    mean_value = jnp.mean(values, axis=-1, keepdims=True)
    centred = values - mean_value
    spread = jnp.mean(centred * centred, axis=-1, keepdims=True)
    return centred * lax.rsqrt(spread + EPS) * gain_row + bias_row


def remote(src, dst, send, recv, sp=None, tp=None):
    target = {}
    if sp is not None:
        target["sp"] = sp
    if tp is not None:
        target["tp"] = tp
    return pltpu.make_async_remote_copy(
        src_ref=src,
        dst_ref=dst,
        send_sem=send,
        recv_sem=recv,
        device_id=target,
        device_id_type=pl.DeviceIdType.MESH,
    )


def pair_columns(values, pair, low_half):
    rows = values.shape[0]
    first = jnp.broadcast_to(values[:, 2 * pair : 2 * pair + 1], (rows, 128))
    second = jnp.broadcast_to(values[:, 2 * pair + 1 : 2 * pair + 2], (rows, 128))
    return jnp.where(low_half[:rows], first, second)


def fused_kernel(n_sp, n_tp, cap, *refs):
    hbm, out, refs = refs[:24], refs[24], refs[25:]
    loaded, refs = refs[:21], refs[21:]
    (x, b, c, gate, logits, extra, fx, fb, fc, bias, rate, direct, gns, resid) = loaded[:14]
    (n1s, n1b, routes, weights, n2s, n2b, wout) = loaded[14:]
    wg, wu, wd = hbm[21:]
    (
        tail_x,
        tail_b,
        tail_c,
        ext_x,
        ext_b,
        ext_c,
        dec_src,
        dec_recv,
        sl_src,
        sl_recv,
        pf_src,
        pf_recv,
        xs,
        xw,
        cb,
        cc,
        ysg,
        ersg,
        added,
        rows_out,
        partial,
        relayed,
        arrived,
        mid,
        outgoing,
        received,
        answers,
        returned,
        tokens,
        hidden,
        summed,
        wg_v,
        wu_v,
        wd_v,
        detour,
        load_sems,
        tail_sems,
        dec_sems,
        sl_sems,
        pf_sems,
        tp_sems,
        w_first,
        w_recv,
        w_relay,
        w_side,
        w_help,
        there,
        back,
    ) = refs
    me = lax.axis_index("sp")
    col = lax.axis_index("tp")
    core = lax.rem(me, 2)
    chip = lax.div(me, 2)
    n_chips = n_sp // 2
    parity = lax.rem(chip, 2)
    sibling = me + 1 - 2 * core
    helper = 2 * (chip + 1 - 2 * parity) + core

    def roles(shift):
        role = lax.rem(col + shift, n_tp)
        partner = role + 1 - 2 * lax.rem(role, 2)
        places = [lax.rem(r - shift + n_tp, n_tp) for r in (partner, 3 - role, 3 - partner)]
        return lax.div(role, 2) == core, *places

    home, beside, across_x, last_place = roles(parity)
    helps, helped_beside, helped_place, _ = roles(1 - parity)

    def crossed(shift):
        return lax.rem(3 - col - 2 * shift + n_tp, n_tp)
    moves = tuple(enumerate(((wg, wg_v), (wu, wu_v), (wd, wd_v))))
    length, width = x.shape
    n_blocks = length // BLOCK
    pairs = width // 128
    groups = b.shape[1] // STATE_WIDTH
    group_width = width // groups
    n_rows, features = mid.shape
    slots = n_sp * cap

    loads = [
        pltpu.make_async_copy(hbm[i], loaded[i], load_sems.at[i]) for i in range(len(loaded))
    ]
    order = (4, 5, 9, 10, 0, 1, 6, 7, 11, 2, 8, 3, 12, 20, 13, 14, 15, 16, 17, 18, 19)
    for i in order:
        loads[i].start()
    barrier = pltpu.get_barrier_semaphore()

    def greet(sp, tp):
        pl.semaphore_signal(
            barrier, inc=1, device_id={"sp": sp, "tp": tp}, device_id_type=pl.DeviceIdType.MESH
        )

    def greet_column(d, carry):
        greet(lax.rem(me + d, n_sp), col)
        return carry

    def greet_plane(q, carry):
        greet(2 * lax.rem(chip + q, n_chips) + core, crossed(0))
        greet(2 * lax.rem(chip + q, n_chips) + core, crossed(1))
        return carry

    lax.fori_loop(1, n_sp, greet_column, 0)
    lax.fori_loop(0, n_chips, greet_plane, 0)

    def arrival(m, place):
        block = moves[m][1][1].at[place]
        return pltpu.make_async_copy(block, block, w_recv.at[place, m])

    ahead = 3 * wg.shape[1] // 8

    def first_hop(m):
        src, dst = moves[min(m, 2)][1]
        spans = {2: pl.ds(0, ahead), 3: pl.ds(ahead, wg.shape[1] - ahead)}
        rows = spans.get(m, pl.ds(0, wg.shape[1]))
        target = jnp.where(home, beside, across_x)
        return remote(
            src.at[0, rows],
            dst.at[col, rows],
            w_first.at[m],
            w_recv.at[col, min(m, 2)],
            tp=target,
        )

    cut = wg.shape[1] // 2
    aside = wg.shape[1] - cut

    def relay(m):
        block = moves[m][1][1].at[across_x, pl.ds(0, cut if m < 2 else cut + aside)]
        return remote(block, block, w_relay.at[m], w_recv.at[across_x, m], tp=beside)

    def to_helper(m):
        block = moves[m][1][1].at[across_x, pl.ds(cut, aside)]
        return remote(block, detour.at[m], w_help.at[0, m], w_help.at[1, m], sp=helper)

    def help_on(m):
        block = moves[m][1][1].at[helped_place, pl.ds(cut, aside)]
        return remote(
            detour.at[m],
            block,
            w_help.at[2, m],
            w_recv.at[helped_place, m],
            sp=helper,
            tp=helped_beside,
        )

    def sideways(m, place, src=None):
        block = moves[m][1][1].at[place]
        return remote(
            block if src is None else src,
            block,
            w_side.at[place, m],
            w_recv.at[place, m],
            sp=sibling,
        )

    def start_weights(first, last):
        for m in range(first, last):
            first_hop(m).start()

        @pl.when(home)
        def _():
            for m in range(first, last):
                src, dst = moves[m][1]
                pltpu.make_async_copy(src.at[0], dst.at[col], w_recv.at[col, m]).start()
                sideways(m, col, src.at[0]).start()

    low_half = lax.broadcasted_iota(jnp.int32, (BLOCK, 128), 1) < 64
    row_id = lax.broadcasted_iota(jnp.int32, (BLOCK, BLOCK), 0)
    lane_id = lax.broadcasted_iota(jnp.int32, (BLOCK, BLOCK), 1)
    causal = row_id >= lane_id
    lower = causal.astype(F32)

    for i in (4, 5, 9, 10):
        loads[i].wait()
    raw = logits[...].T + bias[...]
    steps = jnp.maximum(raw, 0.0) + jnp.log(1.0 + jnp.exp(-jnp.abs(raw)))
    decay = -steps * jnp.exp(rate[...]) + extra[...].T
    running = [
        dot(lower, decay[BLOCK * k : BLOCK * (k + 1)], precision=lax.Precision.HIGHEST)
        for k in range(n_blocks)
    ]
    totals = [r[BLOCK - 1 : BLOCK] for r in running]
    whole = functools.reduce(lambda p, q: p + q, totals)
    for j in range(pairs):
        dec_src[j] = pair_columns(whole, j, low_half)

    for i in (0, 1, 6, 7):
        loads[i].wait()
    ext_x[8:, :] = x[...].astype(F32)
    ext_b[8:, :] = b[...].astype(F32)

    def conv(ext, taps, k, j):
        lanes = slice(128 * j, 128 * (j + 1))
        total = None
        for i in range(4):
            start = BLOCK * k + 5 + i
            term = taps[i : i + 1, lanes].astype(F32) * ext[start : start + BLOCK, lanes]
            total = term if total is None else total + term
        return silu(total)

    def inputs_of_block(k):
        rows = slice(BLOCK * k, BLOCK * (k + 1))
        for g in range(groups):
            cb[rows, 128 * g : 128 * (g + 1)] = conv(ext_b, fb, k, g).astype(BF16)
        to_end = steps[rows] * jnp.exp(totals[k] - running[k])
        for j in range(pairs):
            lanes = slice(128 * j, 128 * (j + 1))
            value = conv(ext_x, fx, k, j)
            ysg[rows, lanes] = value
            xw[rows, lanes] = (value * pair_columns(to_end, j, low_half)).astype(BF16)
        for g in range(groups):
            lanes = slice(group_width * g, group_width * (g + 1))
            added[k, :, lanes] = dot(
                cb[rows, 128 * g : 128 * (g + 1)], xw[rows, lanes], ((0,), (0,))
            )

    for k in range(n_blocks - 1, 0, -1):
        inputs_of_block(k)

    loads[2].wait()
    pl.semaphore_wait(barrier, n_sp - 1 + 2 * n_chips)
    after = lax.rem(me + 1, n_sp)
    tails = [
        remote(v.at[pl.ds(length - 8, 8)], t, tail_sems.at[0, i], tail_sems.at[1, i], sp=after)
        for i, (v, t) in enumerate(((x, tail_x), (b, tail_b), (c, tail_c)))
    ]
    for copy in tails:
        copy.start()
    start_weights(0, 3)
    def send_decay(d, carry):
        target = lax.rem(me + d, n_sp)
        remote(
            dec_src.at[lax.rem(target, pairs)],
            dec_recv.at[d],
            dec_sems.at[0],
            dec_sems.at[1],
            sp=target,
        ).start()
        return carry

    own_decay = pltpu.make_async_copy(
        dec_src.at[lax.rem(me, pairs)], dec_recv.at[0], dec_sems.at[1]
    )
    own_decay.start()
    lax.fori_loop(1, n_sp, send_decay, 0)

    keep = [
        jnp.concatenate([pair_columns(jnp.exp(t), j, low_half) for j in range(pairs)], axis=1)
        for t in totals
    ]

    for copy in tails:
        copy.wait()
    has_tail = (me > 0).astype(F32)
    ext_x[0:8, :] = tail_x[...].astype(F32) * has_tail
    ext_b[0:8, :] = tail_b[...].astype(F32) * has_tail
    inputs_of_block(0)

    for i in range(STATE_WIDTH // 16):
        for j in range(pairs):
            lanes = slice(128 * j, 128 * (j + 1))
            state = added[0, 16 * i : 16 * (i + 1), lanes]
            for k in range(1, n_blocks):
                state = keep[k][:, lanes] * state + added[k, 16 * i : 16 * (i + 1), lanes]
            sl_src[pairs * i + j] = state.astype(BF16)

    def send_slice(d, carry):
        target = lax.rem(me + d, n_sp)
        remote(sl_src.at[target], sl_recv.at[d], sl_sems.at[0], sl_sems.at[1], sp=target).start()
        return carry

    own_slice = pltpu.make_async_copy(sl_src.at[me], sl_recv.at[0], sl_sems.at[1])
    own_slice.start()
    lax.fori_loop(1, n_sp, send_slice, 0)

    for i in (8, 11, 3):
        loads[i].wait()
    ext_c[8:, :] = c[...].astype(F32)
    ext_c[0:8, :] = tail_c[...].astype(F32) * has_tail
    for k in range(n_blocks):
        rows = slice(BLOCK * k, BLOCK * (k + 1))
        across = running[k].T
        grown = jnp.exp(running[k])
        for g in range(groups):
            lanes_g = slice(128 * g, 128 * (g + 1))
            cc[rows, lanes_g] = conv(ext_c, fc, k, g).astype(BF16)
            products = dot(cc[rows, lanes_g], cb[rows, lanes_g], ((1,), (1,)))
            for j in range(g * pairs // groups, (g + 1) * pairs // groups):
                lanes = slice(128 * j, 128 * (j + 1))
                weighed = []
                for h in (2 * j, 2 * j + 1):
                    spread = running[k][:, h : h + 1] - across[h : h + 1, :]
                    factors = jnp.exp(jnp.where(causal, spread, -jnp.inf))
                    weighed.append((products * factors).astype(BF16))
                value = ysg[rows, lanes]
                inputs = (value * pair_columns(steps[rows], j, low_half)).astype(BF16)
                zero = jnp.zeros_like(inputs)
                stacked = jnp.concatenate(
                    [jnp.where(low_half, inputs, zero), jnp.where(low_half, zero, inputs)], axis=0
                )
                within = dot(jnp.concatenate(weighed, axis=1), stacked)
                opened = silu(gate[rows, lanes].astype(F32))
                passed = value * pair_columns(direct[...], j, low_half)
                ysg[rows, lanes] = (passed + within) * opened
                ersg[rows, lanes] = pair_columns(grown, j, low_half) * opened

    pltpu.make_async_copy(dec_recv, dec_recv, dec_sems.at[1]).wait()
    pltpu.make_async_copy(sl_recv, sl_recv, sl_sems.at[1]).wait()

    def scan_step(j, state):
        d = lax.rem(me - j + n_sp, n_sp)
        pf_src[j] = state.astype(BF16)
        return jnp.exp(dec_recv[d]) * state + sl_recv[d].astype(F32)

    lax.fori_loop(0, n_sp, scan_step, jnp.zeros((16, 128), F32))

    def send_prefix(d, carry):
        target = lax.rem(me + d, n_sp)
        remote(pf_src.at[target], pf_recv.at[me], pf_sems.at[0], pf_sems.at[1], sp=target).start()
        return carry

    own_prefix = pltpu.make_async_copy(pf_src.at[me], pf_recv.at[me], pf_sems.at[1])
    own_prefix.start()
    lax.fori_loop(1, n_sp, send_prefix, 0)
    for i in (12, 20, 13, 14, 15, 16, 17, 18, 19):
        loads[i].wait()

    named = routes[...].astype(F32).T.astype(jnp.int32)
    distance = lax.shift_right_logical(named, 1) - chip
    distance = jnp.where(distance < 0, distance + n_chips, distance)
    near = lax.shift_right_logical(distance, 2)
    role = (col + (lax.shift_right_logical(named, 1) & 1)) & 3
    block = 4 * near + 2 * (distance & 1)
    block = block + jnp.where((named & 1) == lax.shift_right_logical(role, 1), 0, 1)
    block = block + (n_sp // 2) * lax.shift_right_logical(distance & 3, 1)
    shares = weights[...].T
    expert_id = lax.broadcasted_iota(jnp.int32, (n_rows, n_sp), 1)
    hits = [(expert_id == block[:, k : k + 1]).astype(F32) for k in range(2)]
    r_id = lax.broadcasted_iota(jnp.int32, (n_rows, n_rows), 0)
    s_id = lax.broadcasted_iota(jnp.int32, (n_rows, n_rows), 1)
    before = dot((s_id < r_id).astype(BF16), (hits[0] + hits[1]).astype(BF16))
    slot_id = lax.broadcasted_iota(jnp.int32, (n_rows, slots), 1)
    at_slot = []
    for k in range(2):
        rank = jnp.sum(before * hits[k], axis=1, keepdims=True).astype(jnp.int32)
        at_slot.append(slot_id == block[:, k : k + 1] * cap + rank)
    chosen = (at_slot[0] | at_slot[1]).astype(F32).astype(BF16)
    share = jnp.where(at_slot[0], shares[:, 0:1], 0.0) + jnp.where(at_slot[1], shares[:, 1:2], 0.0)
    coarse = share.astype(BF16)
    fine = (share - coarse.astype(F32)).astype(BF16)
    gain = gns[...].astype(F32).reshape(1, width)

    pltpu.make_async_copy(pf_recv, pf_recv, pf_sems.at[1]).wait()

    incoming = jnp.concatenate(
        [
            jnp.concatenate([pf_recv[pairs * i + j] for j in range(pairs)], axis=1)
            for i in range(STATE_WIDTH // 16)
        ],
        axis=0,
    ).astype(F32)
    for k in range(n_blocks):
        rows = slice(BLOCK * k, BLOCK * (k + 1))
        for g in range(groups):
            lanes = slice(group_width * g, group_width * (g + 1))
            carried = dot(cc[rows, 128 * g : 128 * (g + 1)], incoming[:, lanes].astype(BF16))
            gated = ysg[rows, lanes] + carried * ersg[rows, lanes]
            power = jnp.mean(gated * gated, axis=-1, keepdims=True)
            rows_out[rows, lanes] = (gated * lax.rsqrt(power + EPS) * gain[:, lanes]).astype(BF16)
        if k + 1 < n_blocks:
            incoming = keep[k] * incoming + added[k]

    @pl.when(home)
    def _():
        for m in range(2):
            arrival(m, across_x).wait()
            to_helper(m).start()

    part = length // n_tp
    half = part // 2
    right, left = lax.rem(col + 1, n_tp), lax.rem(col + n_tp - 1, n_tp)
    opposite = lax.rem(col + 2, n_tp)

    def project(target):
        start = pl.multiple_of(target * part, part)
        for q in range(4):
            lanes = slice(512 * q, 512 * (q + 1))
            partial[pl.ds(start, part), lanes] = dot(
                rows_out[pl.ds(start, part), :], wout[:, lanes]
            ).astype(BF16)

    def half_of(target, which):
        return pl.ds(pl.multiple_of(target * part + which * half, half), half)

    def pass_on(i, rows, dst, target):
        return remote(
            partial.at[rows], dst, tp_sems.at[0, i], tp_sems.at[1, i], tp=target
        )

    project(opposite)
    outward = [
        pass_on(0, half_of(opposite, 0), relayed.at[0], right),
        pass_on(1, half_of(opposite, 1), relayed.at[1], left),
    ]
    for copy in outward:
        copy.start()
    project(right)
    direct_right = pass_on(2, half_of(right, 1), arrived.at[0], right)
    direct_right.start()
    project(left)
    direct_left = pass_on(3, half_of(left, 0), arrived.at[1], left)
    direct_left.start()
    outward[0].wait()
    rows = half_of(right, 0)
    partial[rows, :] = (partial[rows, :].astype(F32) + relayed[0].astype(F32)).astype(BF16)
    joined_right = pass_on(4, rows, arrived.at[2], right)
    joined_right.start()
    outward[1].wait()
    rows = half_of(left, 1)
    partial[rows, :] = (partial[rows, :].astype(F32) + relayed[1].astype(F32)).astype(BF16)
    joined_left = pass_on(5, rows, arrived.at[3], left)
    joined_left.start()
    first_hop(3).start()
    project(col)

    def pass_weights(first, last):
        @pl.when(home)
        def _():
            for m in range(first, last):
                if m == 2:
                    arrival(m, across_x).wait()
                relay(m).start()
                sideways(m, across_x).start()
                arrival(m, beside).wait()
                sideways(m, beside).start()

    def help_with(m):
        @pl.when(helps)
        def _():
            to_helper(m).wait_recv()
            help_on(m).start()

    pass_weights(0, 2)

    for copy in (direct_right, direct_left, joined_right, joined_left):
        copy.wait()
    for which in range(2):
        rows = half_of(col, which)
        span = slice(half * which, half * (which + 1))
        mixed = partial[rows, :].astype(F32)
        mixed = mixed + arrived[1 - which].astype(F32) + arrived[2 + which].astype(F32)
        mid[span, :] = layer_norm(
            ALPHA * resid[span, :].astype(F32) + mixed, n1s[...], n1b[...]
        ).astype(BF16)

    for q in range(4):
        lanes = slice(512 * q, 512 * (q + 1))
        piece = dot(chosen, mid[:, lanes], ((0,), (0,))).astype(BF16)
        outgoing[:, 4 * q : 4 * (q + 1), :] = piece.reshape(slots, 4, 128)

    def place_of(d):
        r = lax.rem(d, n_sp // 2)
        quarter = 4 * lax.div(r, 4) + 2 * lax.div(d, n_sp // 2) + lax.rem(lax.div(r, 2), 2)
        return quarter, lax.rem(d, 2)

    def plane(crossing, shift):
        return col + crossing * (crossed(shift) - col)

    n_parts = 2
    blocks = n_sp // n_parts
    piece_rows = blocks * cap

    def send_tokens(d, carry):
        quarter, crossing = place_of(d)
        target = lax.rem(chip + quarter, n_chips)
        span = pl.ds(cap * d, cap)
        remote(
            outgoing.at[span],
            received.at[span],
            there.at[0],
            there.at[1 + lax.div(d, blocks)],
            sp=2 * target + core,
            tp=plane(crossing, lax.rem(target, 2)),
        ).start()
        return carry

    def send_answers(d, carry):
        quarter, crossing = place_of(d)
        span = pl.ds(cap * d, cap)
        remote(
            answers.at[span],
            returned.at[span],
            back.at[0],
            back.at[1],
            sp=2 * lax.rem(chip - quarter + n_chips, n_chips) + core,
            tp=plane(crossing, parity),
        ).start()
        return carry

    own = pltpu.make_async_copy(outgoing.at[pl.ds(0, cap)], received.at[pl.ds(0, cap)], there.at[1])
    own.start()
    lax.fori_loop(1, n_sp, send_tokens, 0)

    def hidden_part(p, place):
        rows = slice(piece_rows * p, piece_rows * (p + 1))
        opened = dot(tokens[rows, :], wg_v[place])
        upward = dot(tokens[rows, :], wu_v[place])
        hidden[place, rows, :] = (silu(opened) * upward).astype(BF16)

    early = (col, beside, across_x)

    def early_hidden(p, i, carry):
        hidden_part(p, jnp.where(i == 0, early[0], jnp.where(i == 1, early[1], early[2])))
        return carry

    def down(p, place, features_here):
        rows = slice(piece_rows * p, piece_rows * (p + 1))
        return dot(hidden[place, rows, :], wd_v[place, features_here, :], ((1,), (1,)))

    def early_down(p):
        def chunk(q, carry):
            here = pl.ds(pl.multiple_of(256 * q, 256), 256)
            rows = slice(piece_rows * p, piece_rows * (p + 1))
            summed[q, rows, :] = functools.reduce(
                lambda u, v: u + v, [down(p, place, here) for place in early]
            )
            return carry

        lax.fori_loop(0, features // 256, chunk, 0)

    def late_down(p):
        rows = slice(piece_rows * p, piece_rows * (p + 1))
        for q in range(features // 256):
            total = summed[q, rows, :] + down(p, last_place, slice(256 * q, 256 * (q + 1)))
            answers[rows, 2 * q : 2 * q + 2, :] = total.astype(BF16).reshape(piece_rows, 2, 128)

    help_with(0)
    help_with(1)
    pass_weights(2, 3)

    @pl.when(home)
    def _():
        for m in range(3):
            arrival(m, col).wait()

    @pl.when(jnp.logical_not(home))
    def _():
        for m in range(3):
            for place in early:
                arrival(m, place).wait()

    def wait_last(first, last):
        for m in range(first, last):
            arrival(m, last_place).wait()

            @pl.when(home)
            def _():
                sideways(m, last_place).start()

    for p in range(n_parts):
        span = pl.ds(piece_rows * p, piece_rows)
        pltpu.make_async_copy(received.at[span], received.at[span], there.at[1 + p]).wait()
        tokens[span, :] = received[span].reshape(piece_rows, features)
        lax.fori_loop(0, 3, functools.partial(early_hidden, p), 0)
        early_down(p)
        if p == 0:
            wait_last(0, 2)
        hidden_part(p, last_place)
        if p == 0:
            wait_last(2, 3)
        late_down(p)
        if p == 0:
            own = pltpu.make_async_copy(
                answers.at[pl.ds(0, cap)], returned.at[pl.ds(0, cap)], back.at[1]
            )
            own.start()
        lax.fori_loop(max(1, blocks * p), blocks * (p + 1), send_answers, 0)

    pltpu.make_async_copy(returned, returned, back.at[1]).wait()
    back_rows = returned[...].reshape(slots, features)
    ffn = dot(coarse, back_rows) + dot(fine, back_rows)
    out[...] = layer_norm(ALPHA * mid[...].astype(F32) + ffn, n2s[...], n2b[...]).astype(BF16)

    def wait_sent(src, sem):
        remote(src, src, sem, sem, sp=after).wait_send()

    wait_sent(dec_recv.at[pl.ds(0, n_sp - 1)], dec_sems.at[0])
    wait_sent(sl_src.at[pl.ds(0, n_sp - 1)], sl_sems.at[0])
    wait_sent(pf_src.at[pl.ds(0, n_sp - 1)], pf_sems.at[0])
    rest = pl.ds(cap, slots - cap)
    wait_sent(outgoing.at[rest], there.at[0])
    wait_sent(answers.at[rest], back.at[0])
    for m in range(4):
        first_hop(m).wait_send()

    @pl.when(home)
    def _():
        for m in range(3):
            relay(m).wait_send()
            if m < 2:
                to_helper(m).wait_send()
            for place in range(n_tp):
                sideways(m, place).wait_send()

    @pl.when(helps)
    def _():
        for m in range(2):
            help_on(m).wait_send()


def shards(n_sp, n_tp, *arguments):
    (
        head_input_values,
        group_input_vectors,
        group_readout_vectors,
        output_gate_values,
        step_size_logits,
        extra_log_decay,
        head_input_filter,
        input_vector_filter,
        readout_vector_filter,
        step_size_bias,
        head_rate_logarithm,
        direct_path_weight,
        group_norm_scale,
        mixer_output_weight,
        residual,
        first_norm_scale,
        first_norm_bias,
        routes,
        routing_weight,
        expert_gate_weight,
        expert_up_weight,
        expert_down_weight,
        final_norm_scale,
        final_norm_bias,
    ) = arguments
    length, width = head_input_values.shape
    state_lanes = group_input_vectors.shape[1]
    rows_here, features = residual.shape
    n_blocks = length // BLOCK
    pairs = width // 128
    slices = (n_sp, 16, 128)
    vmem = pl.BlockSpec(memory_space=pltpu.VMEM)
    anywhere = pl.BlockSpec(memory_space=pl.ANY)
    dma = pltpu.SemaphoreType.DMA
    experts = n_sp * expert_gate_weight.shape[0]
    cap = max(2, rows_here * routes.shape[1] * 5 // (3 * experts))
    slots = n_sp * cap
    tiles = (slots, features // 128, 128)
    part = expert_gate_weight.shape[2]
    operands = (
        head_input_values,
        group_input_vectors,
        group_readout_vectors,
        output_gate_values,
        step_size_logits.T,
        extra_log_decay.T,
        head_input_filter,
        input_vector_filter,
        readout_vector_filter,
        step_size_bias.reshape(1, -1),
        head_rate_logarithm.reshape(1, -1),
        direct_path_weight.reshape(1, -1),
        group_norm_scale,
        residual,
        first_norm_scale.reshape(1, -1),
        first_norm_bias.reshape(1, -1),
        routes.T,
        routing_weight.T,
        final_norm_scale.reshape(1, -1),
        final_norm_bias.reshape(1, -1),
        mixer_output_weight,
        expert_gate_weight,
        expert_up_weight,
        expert_down_weight,
    )
    return pl.pallas_call(
        functools.partial(fused_kernel, n_sp, n_tp, cap),
        out_shape=jax.ShapeDtypeStruct((rows_here, features), BF16),
        in_specs=[anywhere] * len(operands),
        out_specs=vmem,
        scratch_shapes=[
            *(pltpu.VMEM(v.shape, v.dtype) for v in operands[:21]),
            pltpu.VMEM((8, width), BF16),
            pltpu.VMEM((8, state_lanes), BF16),
            pltpu.VMEM((8, state_lanes), BF16),
            pltpu.VMEM((length + 8, width), F32),
            pltpu.VMEM((length + 8, state_lanes), F32),
            pltpu.VMEM((length + 8, state_lanes), F32),
            pltpu.VMEM((pairs, 1, 128), F32),
            pltpu.VMEM((n_sp, 1, 128), F32),
            pltpu.VMEM(slices, BF16),
            pltpu.VMEM(slices, BF16),
            pltpu.VMEM(slices, BF16),
            pltpu.VMEM(slices, BF16),
            pltpu.VMEM((length, width), BF16),
            pltpu.VMEM((length, width), BF16),
            pltpu.VMEM((length, state_lanes), BF16),
            pltpu.VMEM((length, state_lanes), BF16),
            pltpu.VMEM((length, width), F32),
            pltpu.VMEM((length, width), F32),
            pltpu.VMEM((n_blocks, STATE_WIDTH, width), F32),
            pltpu.VMEM((length, width), BF16),
            pltpu.VMEM((length, features), BF16),
            pltpu.VMEM((2, rows_here // 2, features), BF16),
            pltpu.VMEM((4, rows_here // 2, features), BF16),
            pltpu.VMEM((rows_here, features), BF16),
            pltpu.VMEM(tiles, BF16),
            pltpu.VMEM(tiles, BF16),
            pltpu.VMEM(tiles, BF16),
            pltpu.VMEM(tiles, BF16),
            pltpu.VMEM((slots, features), BF16),
            pltpu.VMEM((n_tp, slots, part), BF16),
            pltpu.VMEM((features // 256, slots, 256), F32),
            pltpu.VMEM((n_tp, features, part), BF16),
            pltpu.VMEM((n_tp, features, part), BF16),
            pltpu.VMEM((n_tp, features, part), BF16),
            pltpu.VMEM((2, features // 2, part), BF16),
            dma((21,)),
            dma((2, 3)),
            dma((2,)),
            dma((2,)),
            dma((2,)),
            dma((2, 6)),
            dma((4,)),
            dma((n_tp, 3)),
            dma((3,)),
            dma((n_tp, 3)),
            dma((3, 2)),
            dma((3,)),
            dma((2,)),
        ],
        compiler_params=pltpu.CompilerParams(
            vmem_limit_bytes=VMEM_LIMIT, has_side_effects=True, collective_id=0
        ),
        name="fused",
    )(*operands)


def solution(mesh):
    every = P(("sp", "tp"), None)
    placed = (
        *([P("sp", "tp")] * 6),
        *([P(None, "tp")] * 3),
        *([P("tp")] * 4),
        P("tp", None),
        every,
        P(),
        P(),
        every,
        every,
        *([P("sp", None, "tp")] * 3),
        P(),
        P(),
    )
    return jax.shard_map(
        functools.partial(shards, mesh.shape["sp"], mesh.shape["tp"]),
        mesh=mesh,
        in_specs=placed,
        out_specs=every,
        check_vma=False,
    )
```
